256 devices in a mesh: ep: 64 (over z, x, core), tp: 4 (over y).
Axes of the slice: x: 4, y: 4, z: 8, core: 2. Of those that a mesh axis runs over, the one named last changes fastest.
Arguments:
- mixer_input: bfloat16 [16384, 2048], P('ep'), may hold values from -6 to 6
- mixer_gain: float32 [2048], replicated, may hold values from 0.1 to 8
- query_one: bfloat16 [2048, 512], P(None, 'tp'), may hold values from -0.1875 to 0.1875
- query_two: bfloat16 [2048, 512], P(None, 'tp'), may hold values from -0.1875 to 0.1875
- key_one: bfloat16 [2048, 256], P(None, 'tp'), may hold values from -0.1875 to 0.1875
- key_two: bfloat16 [2048, 256], P(None, 'tp'), may hold values from -0.1875 to 0.1875
- value_weight: bfloat16 [2048, 512], P(None, 'tp'), may hold values from -0.125 to 0.125
- lambdas: float32 [8], P('tp'), may hold values from 0.3 to 0.8
- head_gain: float32 [128], replicated, may hold values from 0.1 to 1.9
- output_weight: bfloat16 [1024, 2048], P('tp'), may hold values from -0.1875 to 0.1875
- expert_input: bfloat16 [32768, 2048], P(('ep', 'tp')), may hold values from -6 to 6
- expert_gain: float32 [2048], replicated, may hold values from 0.1 to 1.9
- routes: int32 [32768, 2], P(('ep', 'tp')), may hold values from 0 to 63, all different within a row; in each aligned block of 128 rows (0 to 127, 128 to 255, ...) at most 5 rows name the same one
- route_weight: float32 [32768, 2], P(('ep', 'tp')), may hold values from 0.2 to 1
- expert_gate: bfloat16 [64, 2048, 1024], P('ep', None, 'tp'), may hold values from -0.125 to 0.125
- expert_up: bfloat16 [64, 2048, 1024], P('ep', None, 'tp'), may hold values from -0.125 to 0.125
- expert_down: bfloat16 [64, 1024, 2048], P('ep', 'tp'), may hold values from -0.1875 to 0.1875
- shared_gate: bfloat16 [2048, 512], P(None, 'tp'), may hold values from -0.125 to 0.125
- shared_up: bfloat16 [2048, 512], P(None, 'tp'), may hold values from -0.125 to 0.125
- shared_down: bfloat16 [512, 2048], P('tp'), may hold values from -0.25 to 0.25
Outputs:
- mixer_output: bfloat16 [16384, 2048], P(('ep', 'tp'))
- expert_output: bfloat16 [32768, 2048], P(('ep', 'tp'))
The draws below stay inside these ranges and needn't reach their ends.
Inputs may be any that keep to these rules, and one draw needn't show every extreme that they name: `routes`: each row names 2 different experts; in the rows of one device no expert is named by more than 5 rows, and some device names some expert exactly 5 times.
All inputs are finite; a program needn't handle non-finite values.
Results may differ from the reference program's by a relative error of at most 0.014.
The reference program's roundings to bfloat16 on the way count: a program that leaves them out, or rounds other values in their place, can miss the bound.
Values may be sent and summed in bfloat16 or wider, within the bound.
A program may use at most 128 MiB of HBM per device.

```python
import math
import jax
import jax.numpy as jnp
import numpy as np
from jax import lax

D = 2048
HEADS = 8
KV_HEADS = 4
HEAD = 64
VDIM = 128
EFF = 1024
SFF = 512
TOP = 2
EXPERTS = 64
ROWS = 128
CAP = 5
SEQ_LEN = 16384
TOKENS = 32768
N_EP = 64
N_TP = 4


def draw_mixer_gain(key, part):
    return jnp.clip(1.0 + 0.18 * jax.random.normal(key, (D,), jnp.float32), 0.1, 1.9)


def shard_levels(stream_key, shape, cuts, least, largest):
    def one(position, blocks):
        draws = jax.random.uniform(jax.random.fold_in(jax.random.fold_in(stream_key, 6), position), (blocks,), jnp.float32, least / len(cuts), largest / len(cuts))
        return jnp.repeat(jnp.exp(draws), shape[position] // blocks).reshape((-1,) + (1,) * (len(shape) - position - 1))

    level = one(*cuts[0])
    for cut in cuts[1:]:
        level = level * one(*cut)
    return level


def deal_out(own_key, own, number, rows, number_of, top, most, slope):
    sequence = jax.random.permutation(own_key, number_of)
    crowded, common = shares(number_of, rows * top, most, slope, True), shares(number_of, rows * top, most, slope, False)
    places = jnp.arange(number_of)

    def named(tallies, offset_by):
        used = int((tallies > 0).sum())
        fixed = max(1, used // 4)
        moved = fixed + (places - fixed + offset_by * (used - fixed)) % max(1, number_of - fixed)
        return jnp.zeros((number_of,), jnp.int32).at[sequence[jnp.where(places < fixed, places, moved)]].set(jnp.asarray(tallies, jnp.int32))

    tallies = jnp.where(number % 4 == 0, named(crowded, number // 4), named(common, number - number // 4 - 1))
    mixed = jax.random.permutation(jax.random.fold_in(own, 3), number_of)
    giver, sink = mixed[0:number_of // 2 * 2:2], mixed[1:number_of // 2 * 2:2]
    slack = jnp.minimum(tallies[giver] - 1, most - tallies[sink]) // 2
    slack = jnp.where((giver == sequence[0]) | (sink == sequence[0]) | (tallies[sink] == 0), 0, jnp.maximum(slack, 0))
    moved = jax.random.randint(jax.random.fold_in(own, 4), (number_of // 2,), 0, 1 << 20) % (slack + 1)
    tallies = tallies.at[giver].add(-moved).at[sink].add(moved)
    items = jnp.searchsorted(jnp.cumsum(tallies), jnp.arange(rows * top), side="right").astype(jnp.int32)
    listing = items.reshape(top, rows).T
    listing = listing[jax.random.permutation(jax.random.fold_in(own, 1), rows)]
    offset_by = jax.random.randint(jax.random.fold_in(own, 2), (rows, 1), 0, top)
    return jnp.take_along_axis(listing, (jnp.arange(top)[None, :] + offset_by) % top, axis=1)


def shares(count, total, reach, slope, full):
    loads = [(1 << 20) // math.isqrt(standing ** slope) + 1 for standing in range(1, count + 1)]
    largest = reach if full else min(reach, max(-(-total // count), total * loads[0] // sum(loads)))
    least = 1 if total - largest >= count - 1 else 0
    given, surplus = [largest] + [least] * (count - 1), total - largest - least * (count - 1)
    while surplus > 0:
        free = [i for i in range(1, count) if given[i] < largest] or [i for i in range(1, count) if given[i] < reach]
        whole, budget = sum([loads[i] for i in free]), surplus
        for i in free:
            extra = min(reach - given[i], max(1, budget * loads[i] // whole), surplus)
            given[i] = given[i] + extra
            surplus = surplus - extra
    return np.array(given)


def centred(rng, dims, width, most, shards=(), kind=jnp.bfloat16):
    drawn = width * jax.random.normal(rng, dims, jnp.float32)
    if shards:
        drawn = drawn * shard_levels(rng, dims, shards, -0.22, 0.18)
    return jnp.clip(drawn, -most, most).astype(kind)


def setup_inputs(seed: int = 0) -> dict:
    arg_keys = jax.random.split(jax.random.key(seed), 21)
    mixer_input = centred(arg_keys[0], (SEQ_LEN, D), 1.0, 6.0, ((0, 64),))
    mixer_gain = draw_mixer_gain(jax.random.fold_in(arg_keys[20], 71), 0)
    query_one = centred(arg_keys[2], (D, HEADS * HEAD), (D // 2) ** -0.5, 0.1875, ((1, 4),))
    query_two = centred(arg_keys[3], (D, HEADS * HEAD), (D // 2) ** -0.5, 0.1875, ((1, 4),))
    key_one = centred(arg_keys[4], (D, KV_HEADS * HEAD), (D // 2) ** -0.5, 0.1875, ((1, 4),))
    key_two = centred(arg_keys[5], (D, KV_HEADS * HEAD), (D // 2) ** -0.5, 0.1875, ((1, 4),))
    value_weight = centred(arg_keys[6], (D, KV_HEADS * VDIM), D ** -0.5, 0.125, ((1, 4),))
    lambdas = jnp.clip(0.3 + 0.5 * jax.random.uniform(arg_keys[7], (HEADS,), jnp.float32) ** shard_levels(arg_keys[7], (HEADS,), ((0, 4),), -0.2, 0.2), 0.3, 0.8)
    head_gain = jnp.clip(1.0 + 0.18 * jax.random.normal(arg_keys[8], (VDIM,), jnp.float32), 0.1, 1.9)
    output_weight = centred(arg_keys[9], (HEADS * VDIM, D), (HEADS * VDIM) ** -0.5, 0.1875, ((0, 4),))
    expert_input = centred(arg_keys[10], (TOKENS, D), 1.0, 6.0, ((0, 256),))
    expert_gain = jnp.clip(1.0 + 0.18 * jax.random.normal(arg_keys[11], (D,), jnp.float32), 0.1, 1.9)
    routes_keys = jax.random.split(jax.random.fold_in(arg_keys[12], 1), TOKENS // ROWS)
    routes_turns = jax.random.permutation(jax.random.fold_in(arg_keys[12], 3), TOKENS // ROWS)
    routes = jax.vmap(lambda own, number: deal_out(jax.random.fold_in(arg_keys[12], 2), own, number, ROWS, EXPERTS, TOP, CAP, 2))(routes_keys, routes_turns).reshape((TOKENS, TOP))
    route_weight = jnp.clip(jnp.exp(math.log(1.0) - 1.609438 * jax.random.uniform(arg_keys[13], (TOKENS, TOP), jnp.float32) ** shard_levels(arg_keys[13], (TOKENS, TOP), ((0, 256),), -0.2, 0.2)), 0.2, 1.0)
    expert_gate = centred(arg_keys[14], (EXPERTS, D, EFF), D ** -0.5, 0.125, ((0, 64), (2, 4)))
    expert_up = centred(arg_keys[15], (EXPERTS, D, EFF), D ** -0.5, 0.125, ((0, 64), (2, 4)))
    expert_down = centred(arg_keys[16], (EXPERTS, EFF, D), EFF ** -0.5, 0.1875, ((0, 64), (1, 4)))
    shared_gate = centred(arg_keys[17], (D, SFF), D ** -0.5, 0.125, ((1, 4),))
    shared_up = centred(arg_keys[18], (D, SFF), D ** -0.5, 0.125, ((1, 4),))
    shared_down = centred(arg_keys[19], (SFF, D), SFF ** -0.5, 0.25, ((0, 4),))
    return dict(mixer_input=mixer_input, mixer_gain=mixer_gain, query_one=query_one, query_two=query_two, key_one=key_one, key_two=key_two, value_weight=value_weight, lambdas=lambdas, head_gain=head_gain, output_weight=output_weight, expert_input=expert_input, expert_gain=expert_gain, routes=routes, route_weight=route_weight, expert_gate=expert_gate, expert_up=expert_up, expert_down=expert_down, shared_gate=shared_gate, shared_up=shared_up, shared_down=shared_down)


EPS = 1e-06
NEG = -1e+30

def normalize(activations, scaling):
    values = activations.astype(jnp.float32)
    factor = lax.rsqrt(lax.optimization_barrier(jnp.mean(values * values, axis=-1, keepdims=True)) + EPS)
    return (values * factor * scaling).astype(jnp.bfloat16)

def swiglu(inputs, gate_weight, up_weight):
    gated = jnp.dot(inputs, gate_weight, preferred_element_type=jnp.float32)
    lifted = jnp.dot(inputs, up_weight, preferred_element_type=jnp.float32)
    return (jax.nn.silu(gated) * lifted).astype(jnp.bfloat16)

def quarter_sum(hidden, down_weight):
    group_width = hidden.shape[1] // N_TP
    running_sum = jnp.zeros((hidden.shape[0], down_weight.shape[1]), jnp.float32)
    for group_index in range(N_TP):
        partial_product = jnp.dot(hidden[:, group_index * group_width:(group_index + 1) * group_width], down_weight[group_index * group_width:(group_index + 1) * group_width], preferred_element_type=jnp.float32)
        rounded = lax.optimization_barrier(partial_product.astype(jnp.bfloat16))
        running_sum = running_sum + rounded.astype(jnp.float32)
    return running_sum

def attention(mixer_input, mixer_gain, query_one, query_two, key_one, key_two, value_weight, lambdas, head_gain, output_weight):
    normed = normalize(mixer_input, mixer_gain)
    tokens = normed.shape[0]
    group_size = HEADS // KV_HEADS

    def project(weight):
        return jnp.dot(normed, weight, preferred_element_type=jnp.float32).astype(jnp.bfloat16)
    query_first = project(query_one).reshape(tokens, KV_HEADS, group_size, HEAD)
    query_second = project(query_two).reshape(tokens, KV_HEADS, group_size, HEAD)
    key_first = project(key_one).reshape(tokens, KV_HEADS, HEAD).astype(jnp.float32)
    key_second = project(key_two).reshape(tokens, KV_HEADS, HEAD).astype(jnp.float32)
    value_rows = project(value_weight).reshape(tokens, KV_HEADS, VDIM).astype(jnp.float32)
    lambda_grid = lambdas.reshape(KV_HEADS, group_size)[:, :, None, None]
    key_pos = jnp.arange(tokens, dtype=jnp.int32)
    span_rows = min(128, tokens)

    def single_map(queries, key_rows, visible):
        scores = jnp.einsum('qkgd,jkd->kgqj', queries.astype(jnp.float32), key_rows) * HEAD ** (-0.5)
        scores = jnp.where(visible, scores, NEG)
        highest = lax.optimization_barrier(jnp.max(scores, axis=-1, keepdims=True))
        weights = jnp.where(visible, jnp.exp(scores - highest), 0.0)
        totals = lax.optimization_barrier(jnp.sum(weights, axis=-1))
        rounded = lax.optimization_barrier(weights.astype(jnp.bfloat16)).astype(jnp.float32)
        mixed = jnp.einsum('kgqj,jkd->kgqd', rounded, value_rows)
        return mixed / totals[..., None]

    def query_block(block_index):
        offset = (block_index * span_rows).astype(jnp.int32)
        query_pos = offset + jnp.arange(span_rows, dtype=jnp.int32)
        visible = key_pos[None, :] <= query_pos[:, None]
        first_part = single_map(lax.dynamic_slice_in_dim(query_first, offset, span_rows, 0), key_first, visible)
        second_part = single_map(lax.dynamic_slice_in_dim(query_second, offset, span_rows, 0), key_second, visible)
        combined = first_part - lambda_grid * second_part
        factor = lax.rsqrt(lax.optimization_barrier(jnp.mean(combined * combined, axis=-1, keepdims=True)) + EPS)
        normed_heads = (combined * factor * head_gain).astype(jnp.bfloat16)
        return normed_heads.transpose(2, 0, 1, 3).reshape(span_rows, HEADS * VDIM)
    head_rows = lax.map(query_block, jnp.arange(tokens // span_rows, dtype=jnp.int32))
    head_rows = head_rows.reshape(tokens, HEADS * VDIM)
    return quarter_sum(head_rows, output_weight).astype(jnp.bfloat16)

def experts_part(expert_input, expert_gain, routes, route_weight, expert_gate, expert_up, expert_down, shared_gate, shared_up, shared_down):
    normed = normalize(expert_input, expert_gain)
    tokens = normed.shape[0]
    shared_result = quarter_sum(swiglu(normed, shared_gate, shared_up), shared_down)
    flat_routes = routes.reshape(-1).astype(jnp.int32)
    copies = flat_routes.shape[0]
    onehot = (flat_routes[:, None] == jnp.arange(EXPERTS, dtype=jnp.int32)[None, :]).astype(jnp.int32)
    slot_place = lax.optimization_barrier(jnp.sum((jnp.cumsum(onehot, axis=0) - onehot) * onehot, axis=1)).astype(jnp.int32)
    owners = (jnp.arange(copies, dtype=jnp.int32) // TOP).astype(jnp.int32)
    table = jnp.zeros((EXPERTS, N_EP * N_TP * CAP), jnp.int32).at[flat_routes, slot_place].set(owners)

    def one_expert(expert_index):
        chosen = normed[table[expert_index]]
        hidden = swiglu(chosen, expert_gate[expert_index], expert_up[expert_index])
        return quarter_sum(hidden, expert_down[expert_index]).astype(jnp.bfloat16)
    results = lax.map(one_expert, jnp.arange(EXPERTS, dtype=jnp.int32))
    picked = results[flat_routes, slot_place].astype(jnp.float32).reshape(tokens, TOP, -1)
    routed = lax.optimization_barrier(jnp.sum(picked * route_weight[:, :, None], axis=1))
    return (routed + shared_result).astype(jnp.bfloat16)

def reference(mixer_input, mixer_gain, query_one, query_two, key_one, key_two, value_weight, lambdas, head_gain, output_weight, expert_input, expert_gain, routes, route_weight, expert_gate, expert_up, expert_down, shared_gate, shared_up, shared_down):
    mixer_output = attention(mixer_input, mixer_gain, query_one, query_two, key_one, key_two, value_weight, lambdas, head_gain, output_weight)
    expert_output = experts_part(expert_input, expert_gain, routes, route_weight, expert_gate, expert_up, expert_down, shared_gate, shared_up, shared_down)
    return (mixer_output, expert_output)
```

```python
import functools

import jax
import jax.numpy as jnp
from jax import lax
from jax.experimental import pallas as pl
from jax.experimental.pallas import tpu as pltpu
from jax.sharding import PartitionSpec as P

HEAD = 64

EPS = 1e-06
NEG = -1e30
MESH = pl.DeviceIdType.MESH

SPAN = 2


def normalize(activations, scaling):
    values = activations.astype(jnp.float32)
    factor = lax.rsqrt(jnp.mean(values * values, axis=-1, keepdims=True) + EPS)
    return (values * factor * scaling).astype(jnp.bfloat16)


def swap_high(block, axis):
    count = lax.axis_size(axis)
    return lax.ppermute(block, axis, [(i, count - 1 - i) for i in range(count)])


def attention_kernel(rank_ref, low_ref, high_ref, kv_ref, lam_ref, gain_ref, out_ref, query, maxima, totals, weighted):
    shards, block_rows, _ = kv_ref.shape
    rows = block_rows // 2
    half = rows // 2
    span_keys = SPAN * rows
    rank = rank_ref[0]
    zeros = jnp.zeros((HEAD, 2 * half), jnp.bfloat16)
    for which, source in enumerate((low_ref, high_ref)):
        first = jnp.concatenate([source[0:HEAD], source[HEAD : 2 * HEAD]], axis=1)
        second = jnp.concatenate([source[2 * HEAD : 3 * HEAD], source[3 * HEAD : 4 * HEAD]], axis=1)
        query[which, 0, 0:HEAD] = first
        query[which, 0, HEAD : 2 * HEAD] = zeros
        query[which, 1, 0:HEAD] = zeros
        query[which, 1, HEAD : 2 * HEAD] = second

    def block(which, shard, masked, query_start):
        keys = kv_ref[pl.ds(shard, SPAN), 0:rows, :].reshape(span_keys, 2 * HEAD)
        values = [kv_ref[shard + i, rows + j * half : rows + (j + 1) * half, :] for i in range(SPAN) for j in range(2)]
        values = jnp.concatenate(values, axis=1)
        if masked:
            key_pos = shard * rows + lax.broadcasted_iota(jnp.int32, (span_keys, 2 * half), 0)
            lane = lax.broadcasted_iota(jnp.int32, (span_keys, 2 * half), 1)
            query_pos = query_start + jnp.where(lane >= half, lane - half, lane)
            visible = key_pos <= query_pos
        for m in range(2):
            scores = jnp.dot(keys, query[which, m], preferred_element_type=jnp.float32)
            if masked:
                scores = jnp.where(visible, scores, NEG)
            earlier = maxima[which, m]
            latest = jnp.maximum(earlier, jnp.max(scores, axis=0, keepdims=True))
            shrink = jnp.exp(earlier - latest)
            weights = jnp.exp(scores - latest)
            if masked:
                weights = jnp.where(visible, weights, 0.0)
            totals[which, m] = totals[which, m] * shrink + jnp.sum(weights, axis=0, keepdims=True)
            product = jnp.dot(values, weights.astype(jnp.bfloat16), preferred_element_type=jnp.float32)
            weighted[which, m] = weighted[which, m] * shrink + product
            maxima[which, m] = latest

    for which in range(2):
        maxima[which] = jnp.full(maxima.shape[1:], NEG, jnp.float32)
        totals[which] = jnp.zeros(totals.shape[1:], jnp.float32)
        weighted[which] = jnp.zeros(weighted.shape[1:], jnp.float32)
        full = rank if which == 0 else shards - 1 - rank
        steps = full // SPAN

        def step(i, carry, which=which):
            block(which, i * SPAN, False, 0)
            return carry

        lax.fori_loop(0, steps, step, 0)
        block(which, steps * SPAN, True, full * rows + which * half)
        mixed = [weighted[which, m] / totals[which, m] for m in range(2)]
        combined = mixed[0] - lam_ref[...] * mixed[1]
        factor = lax.rsqrt(jnp.mean(combined * combined, axis=0, keepdims=True) + EPS)
        normed = combined * factor * gain_ref[...]
        for head in range(2):
            part = normed[:, head * half : (head + 1) * half]
            out_ref[which, :, head * 128 : (head + 1) * 128] = part.T.astype(jnp.bfloat16)


def attend(rank, low, high, kv, lambdas, head_gain):
    shards, block_rows, _ = kv.shape
    half = block_rows // 4
    value_dim = head_gain.shape[0]
    pairs = shards * half * 2
    lam = jnp.repeat(lambdas, half).reshape(1, 2 * half)
    vmem = pl.BlockSpec(memory_space=pltpu.VMEM)
    return pl.pallas_call(
        attention_kernel,
        out_shape=jax.ShapeDtypeStruct((2, half, 2 * value_dim), jnp.bfloat16),
        in_specs=[pl.BlockSpec(memory_space=pltpu.SMEM)] + [vmem] * 5,
        out_specs=vmem,
        scratch_shapes=[
            pltpu.VMEM((2, 2, 2 * HEAD, 2 * half), jnp.bfloat16),
            pltpu.VMEM((2, 2, 1, 2 * half), jnp.float32),
            pltpu.VMEM((2, 2, 1, 2 * half), jnp.float32),
            pltpu.VMEM((2, 2, value_dim, 2 * half), jnp.float32),
        ],
        cost_estimate=pl.CostEstimate(flops=pairs * 2 * half * 2 * 512, bytes_accessed=kv.size * 2, transcendentals=pairs * 2 * half * 2),
        compiler_params=pltpu.CompilerParams(vmem_limit_bytes=40 * 1024 * 1024),
        name="attend",
    )(rank.reshape(1), low, high, kv, lam, head_gain.reshape(value_dim, 1))


def expert_kernel(rows_ref, gate_ref, up_ref, down_ref, out_ref, total):
    group = pl.program_id(0)
    rows = rows_ref[...]
    gated = jnp.dot(rows, gate_ref[0], preferred_element_type=jnp.float32)
    lifted = jnp.dot(rows, up_ref[0], preferred_element_type=jnp.float32)
    hidden = (gated / (1.0 + jnp.exp(-gated)) * lifted).astype(jnp.bfloat16)
    part = jnp.dot(hidden, down_ref[0], preferred_element_type=jnp.float32)
    part = part.astype(jnp.bfloat16).astype(jnp.float32)

    @pl.when(group == 0)
    def _():
        total[...] = part

    @pl.when(group > 0)
    def _():
        total[...] += part

    @pl.when(group == pl.num_programs(0) - 1)
    def _():
        out_ref[...] = total[...].astype(out_ref.dtype)


def swiglu_groups(rows, gate, up, down, kind, name):
    groups, width, hidden = gate.shape
    count = rows.shape[0]
    return pl.pallas_call(
        expert_kernel,
        out_shape=jax.ShapeDtypeStruct((count, width), kind),
        grid=(groups,),
        in_specs=[
            pl.BlockSpec((count, width), lambda g: (0, 0)),
            pl.BlockSpec((1, width, hidden), lambda g: (g, 0, 0)),
            pl.BlockSpec((1, width, hidden), lambda g: (g, 0, 0)),
            pl.BlockSpec((1, hidden, width), lambda g: (g, 0, 0)),
        ],
        out_specs=pl.BlockSpec((count, width), lambda g: (0, 0)),
        scratch_shapes=[pltpu.VMEM((count, width), jnp.float32)],
        cost_estimate=pl.CostEstimate(flops=groups * count * width * hidden * 6, bytes_accessed=groups * width * hidden * 6, transcendentals=groups * count * hidden),
        compiler_params=pltpu.CompilerParams(vmem_limit_bytes=60 * 1024 * 1024),
        name=name,
    )(rows, gate, up, down)


def weight_kernel(*refs):
    count = (len(refs) - 7) // 2
    sources, targets = refs[:count], refs[count : 2 * count]
    send_own, recv_own, send_on, recv_on, send_pair, recv_pair, local = refs[2 * count :]
    size = lax.axis_size("tp")
    me = lax.axis_index("tp")
    place = lax.axis_index("ep")
    core = lax.rem(place, 2)
    right, left = {"tp": lax.rem(me + 1, size)}, {"tp": lax.rem(me + size - 1, size)}
    other = {"ep": place + 1 - 2 * core}
    sides = (right, left)
    first_shared = count - 3

    barrier = pltpu.get_barrier_semaphore()
    for peer in (right, left, other):
        pl.semaphore_signal(barrier, inc=1, device_id=peer, device_id_type=MESH)
    pl.semaphore_wait(barrier, 3)

    def span_of(i):
        rows = sources[i].shape[0]
        return (rows, 0) if i < first_shared else (rows // 2, core * (rows // 2))

    def piece(ref, i, part):
        rows, start = span_of(i)
        return ref.at[pl.ds(start + part * (rows // 2), rows // 2)]

    def whole(ref, i):
        rows, start = span_of(i)
        return ref.at[pl.ds(start, rows)]

    def send(source, target, send_sem, recv_sem, peer):
        copy = pltpu.make_async_remote_copy(
            src_ref=source, dst_ref=target, send_sem=send_sem, recv_sem=recv_sem, device_id=peer, device_id_type=MESH
        )
        copy.start()
        return copy

    items = tuple(range(first_shared, count)) + tuple(range(first_shared))
    own, onward, pairs = {}, {}, []
    for order in range(2):
        for i in items:
            for side in range(2):
                part = side if order == 0 else 1 - side
                own[side, order, i] = send(
                    piece(sources[i], i, part),
                    piece(targets[i].at[me], i, part),
                    send_own.at[side, order, i],
                    recv_own.at[side, order, i],
                    sides[side],
                )
    kept = []
    for i in items:
        copy = pltpu.make_async_copy(sources[i], targets[i].at[me], local.at[i])
        copy.start()
        kept.append(copy)

    for i in items:
        for side in range(2):
            own[side, 0, i].wait_recv()
            view = piece(targets[i].at[sides[1 - side]["tp"]], i, side)
            onward[side, i] = send(view, view, send_on.at[side, i], recv_on.at[side, i], sides[side])

    def to_other(owner, i, k):
        view = whole(targets[i].at[owner], i)
        pairs.append(send(view, view, send_pair.at[k, i - first_shared], recv_pair.at[k, i - first_shared], other))

    for i in items[:3]:
        for side in range(2):
            own[side, 1, i].wait_recv()
            to_other(sides[1 - side]["tp"], i, side)
    for i in items[:3]:
        for side in range(2):
            onward[side, i].wait_recv()
        to_other(lax.rem(me + 2, size), i, 2)
    for i in items[3:]:
        for side in range(2):
            own[side, 1, i].wait_recv()
            onward[side, i].wait_recv()
    for copy in kept:
        copy.wait()
    for copy in pairs:
        copy.wait_recv()
        copy.wait_send()
    for i in items:
        for side in range(2):
            own[side, 0, i].wait_send()
            own[side, 1, i].wait_send()
            onward[side, i].wait_send()


def gather_weights(*weights):
    size = lax.axis_size("tp")
    hbm = pl.BlockSpec(memory_space=pltpu.HBM)
    dma = pltpu.SemaphoreType.DMA
    count = len(weights)
    return pl.pallas_call(
        weight_kernel,
        out_shape=[jax.ShapeDtypeStruct((size,) + w.shape, w.dtype) for w in weights],
        in_specs=[hbm] * count,
        out_specs=[hbm] * count,
        scratch_shapes=[dma((2, 2, count))] * 2 + [dma((2, count))] * 2 + [dma((3, 3))] * 2 + [dma((count,))],
        cost_estimate=pl.CostEstimate(flops=0, bytes_accessed=300_000_000, transcendentals=0),
        compiler_params=pltpu.CompilerParams(collective_id=0, has_side_effects=True, vmem_limit_bytes=60 * 1024 * 1024),
        name="gather_weights",
    )(*weights)


def body(
    mixer_input,
    mixer_gain,
    query_one,
    query_two,
    key_one,
    key_two,
    value_weight,
    lambdas,
    head_gain,
    output_weight,
    expert_input,
    expert_gain,
    routes,
    route_weight,
    expert_gate,
    expert_up,
    expert_down,
    shared_gate,
    shared_up,
    shared_down,
):
    ep_size = lax.axis_size("ep")
    tp_size = lax.axis_size("tp")
    ep_rank = lax.axis_index("ep")
    mixer_rows, model_width = mixer_input.shape
    half_rows = mixer_rows // 2
    token_rows = expert_input.shape[0]

    gate_all = lax.all_gather(expert_gate[0], "tp")

    normed = normalize(mixer_input, mixer_gain)
    query_cols = query_one.shape[1]
    turned_weight = jnp.concatenate([query_one, query_two, value_weight], axis=1)
    turned = lax.dot_general(turned_weight, normed, (((0,), (1,)), ((), ())), preferred_element_type=jnp.float32)
    keys = jnp.dot(normed, jnp.concatenate([key_one, key_two], axis=1), preferred_element_type=jnp.float32)
    keys = keys.astype(jnp.bfloat16)
    queries = (turned[: 2 * query_cols].astype(jnp.bfloat16) * HEAD ** (-0.5)).astype(jnp.bfloat16)
    values = turned[2 * query_cols :].astype(jnp.bfloat16)
    key_values = jnp.concatenate([keys, values[:, :half_rows], values[:, half_rows:]], axis=0)
    arrived = lax.all_gather(key_values, "ep")
    high_queries = swap_high(queries[:, half_rows:], "ep")

    normed_experts = normalize(expert_input, expert_gain)
    expert_count = expert_gate.shape[0] * ep_size
    top_count = routes.shape[1]
    capacity = max(2, 5 * token_rows * top_count // (4 * expert_count))
    slot_count = expert_count * capacity
    flat_routes = routes.reshape(-1)
    onehot = (flat_routes[:, None] == jnp.arange(expert_count, dtype=jnp.int32)[None, :]).astype(jnp.bfloat16)
    before = jnp.tril(jnp.ones((token_rows * top_count, token_rows * top_count), jnp.bfloat16), -1)
    counts = jnp.dot(before, onehot, preferred_element_type=jnp.float32)
    slot_place = jnp.sum(counts * onehot, axis=1).astype(jnp.int32)
    slot_ids = (flat_routes * capacity + slot_place).reshape(token_rows, top_count)
    slot_match = jnp.arange(slot_count, dtype=jnp.int32)[:, None, None] == slot_ids[None, :, :]
    select = jnp.any(slot_match, axis=2).astype(jnp.bfloat16)
    outgoing = jnp.dot(select, normed_experts, preferred_element_type=jnp.float32).astype(jnp.bfloat16)
    lines = slot_count // ep_size * model_width // 128
    outgoing = outgoing.reshape(ep_size, lines, 128)
    outgoing, high_queries = lax.optimization_barrier((outgoing, high_queries))
    received = lax.all_to_all(outgoing, "ep", split_axis=0, concat_axis=0, tiled=True)

    up_all, down_all, shared_gate_all, shared_up_all, shared_down_all = gather_weights(
        expert_up[0], expert_down[0], shared_gate, shared_up, shared_down
    )

    halves = attend(ep_rank, queries[:, :half_rows], high_queries, arrived, lambdas, head_gain)
    slot_rows = received.reshape(slot_count, model_width)
    routed_result = swiglu_groups(slot_rows, gate_all, up_all, down_all, jnp.bfloat16, "routed")
    shared_result = swiglu_groups(
        normed_experts, shared_gate_all, shared_up_all, shared_down_all, jnp.float32, "shared"
    )
    routed_result = routed_result.reshape(ep_size, lines, 128)
    returned = lax.all_to_all(routed_result, "ep", split_axis=0, concat_axis=0, tiled=True)
    returned, halves, shared_result = lax.optimization_barrier((returned, halves, shared_result))
    returned = returned.reshape(slot_count, model_width)
    picks = slot_ids[:, :, None] == jnp.arange(slot_count, dtype=jnp.int32)[None, None, :]
    picks = picks.astype(jnp.bfloat16)
    routed_total = jnp.zeros((token_rows, model_width), jnp.float32)
    for k in range(top_count):
        picked = jnp.dot(picks[:, k], returned, preferred_element_type=jnp.float32)
        routed_total = routed_total + picked * route_weight[:, k : k + 1]
    high_rows = swap_high(halves[1], "ep")
    head_rows = jnp.concatenate([halves[0], high_rows], axis=0)
    partial = jnp.dot(head_rows, output_weight, preferred_element_type=jnp.float32).astype(jnp.bfloat16)
    partial = partial.reshape(tp_size, mixer_rows // tp_size, model_width)
    tp_rank = lax.axis_index("tp")
    mixer_sum = lax.dynamic_index_in_dim(partial, tp_rank, 0, keepdims=False).astype(jnp.float32)
    for step in range(1, tp_size):
        leaving = lax.dynamic_index_in_dim(partial, lax.rem(tp_rank + step, tp_size), 0, keepdims=False)
        part = lax.ppermute(leaving, "tp", [(i, (i + step) % tp_size) for i in range(tp_size)])
        mixer_sum = mixer_sum + part.astype(jnp.float32)
    mixer_output = mixer_sum.astype(jnp.bfloat16)
    expert_output = (routed_total + shared_result).astype(jnp.bfloat16)
    return (mixer_output, expert_output)


def solution(mesh):
    in_specs = (
        P("ep", None),
        P(),
        P(None, "tp"),
        P(None, "tp"),
        P(None, "tp"),
        P(None, "tp"),
        P(None, "tp"),
        P("tp"),
        P(),
        P("tp", None),
        P(("ep", "tp"), None),
        P(),
        P(("ep", "tp"), None),
        P(("ep", "tp"), None),
        P("ep", None, "tp"),
        P("ep", None, "tp"),
        P("ep", "tp", None),
        P(None, "tp"),
        P(None, "tp"),
        P("tp", None),
    )
    out_specs = (P(("ep", "tp"), None), P(("ep", "tp"), None))
    return jax.shard_map(body, mesh=mesh, in_specs=in_specs, out_specs=out_specs, check_vma=False)
```

```python
import jax
import jax.numpy as jnp
from jax import lax
from jax.experimental import pallas as pl
from jax.experimental.pallas import tpu as pltpu
from jax.sharding import PartitionSpec as P

HEAD = 64

EPS = 1e-06
NEG = -1e30
MESH = pl.DeviceIdType.MESH

SPAN = 2
NX = 4


def normalize(activations, scaling):
    values = activations.astype(jnp.float32)
    factor = lax.rsqrt(jnp.mean(values * values, axis=-1, keepdims=True) + EPS)
    return (values * factor * scaling).astype(jnp.bfloat16)


def attention(rank, shards, rows, high_ref, low_ref, kv_ref, lam_ref, gain_ref, results, query, maxima, totals, weighted):
    half = rows // 2
    span_keys = SPAN * rows
    zeros = jnp.zeros((HEAD, 2 * half), jnp.bfloat16)
    for which, source in enumerate((low_ref, high_ref)):
        first = jnp.concatenate([source[0:HEAD], source[HEAD : 2 * HEAD]], axis=1)
        second = jnp.concatenate([source[2 * HEAD : 3 * HEAD], source[3 * HEAD : 4 * HEAD]], axis=1)
        query[which, 0, 0:HEAD] = first
        query[which, 0, HEAD : 2 * HEAD] = zeros
        query[which, 1, 0:HEAD] = zeros
        query[which, 1, HEAD : 2 * HEAD] = second

    def block(which, chip, masked, query_start):
        keys = kv_ref[chip, :, 0:rows, :].reshape(span_keys, 2 * HEAD)
        values = [kv_ref[chip, i, rows + j * half : rows + (j + 1) * half, :] for i in range(SPAN) for j in range(2)]
        values = jnp.concatenate(values, axis=1)
        if masked:
            key_pos = chip * span_keys + lax.broadcasted_iota(jnp.int32, (span_keys, 2 * half), 0)
            lane = lax.broadcasted_iota(jnp.int32, (span_keys, 2 * half), 1)
            query_pos = query_start + jnp.where(lane >= half, lane - half, lane)
            visible = key_pos <= query_pos
        for m in range(2):
            scores = jnp.dot(keys, query[which, m], preferred_element_type=jnp.float32)
            if masked:
                scores = jnp.where(visible, scores, NEG)
            earlier = maxima[which, m]
            latest = jnp.maximum(earlier, jnp.max(scores, axis=0, keepdims=True))
            shrink = jnp.exp(earlier - latest)
            weights = jnp.exp(scores - latest)
            if masked:
                weights = jnp.where(visible, weights, 0.0)
            totals[which, m] = totals[which, m] * shrink + jnp.sum(weights, axis=0, keepdims=True)
            product = jnp.dot(values, weights.astype(jnp.bfloat16), preferred_element_type=jnp.float32)
            weighted[which, m] = weighted[which, m] * shrink + product
            maxima[which, m] = latest

    for which in (1, 0):
        maxima[which] = jnp.full(maxima.shape[1:], NEG, jnp.float32)
        totals[which] = jnp.zeros(totals.shape[1:], jnp.float32)
        weighted[which] = jnp.zeros(weighted.shape[1:], jnp.float32)
        full = rank if which == 0 else shards - 1 - rank
        steps = full // SPAN

        def step(i, carry, which=which):
            block(which, i, False, 0)
            return carry

        lax.fori_loop(0, steps, step, 0)
        block(which, steps, True, full * rows + which * half)
        mixed = [weighted[which, m] / totals[which, m] for m in range(2)]
        combined = mixed[0] - lam_ref[...] * mixed[1]
        factor = lax.rsqrt(jnp.mean(combined * combined, axis=0, keepdims=True) + EPS)
        normed = combined * factor * gain_ref[...]
        for head in range(2):
            part = normed[:, head * half : (head + 1) * half]
            results[which][0:half, head * 128 : (head + 1) * 128] = part.T.astype(jnp.bfloat16)


def expert_kernel(rows_ref, gate_ref, up_ref, down_ref, out_ref, total):
    group = pl.program_id(0)
    rows = rows_ref[...]
    gated = jnp.dot(rows, gate_ref[0], preferred_element_type=jnp.float32)
    lifted = jnp.dot(rows, up_ref[0], preferred_element_type=jnp.float32)
    hidden = (gated / (1.0 + jnp.exp(-gated)) * lifted).astype(jnp.bfloat16)
    part = jnp.dot(hidden, down_ref[0], preferred_element_type=jnp.float32)
    part = part.astype(jnp.bfloat16).astype(jnp.float32)

    @pl.when(group == 0)
    def _():
        total[...] = part

    @pl.when(group > 0)
    def _():
        total[...] += part

    @pl.when(group == pl.num_programs(0) - 1)
    def _():
        out_ref[...] = total[...].astype(out_ref.dtype)


def swiglu_groups(rows, gate, up, down, kind, name):
    groups, width, hidden = gate.shape
    count = rows.shape[0]
    return pl.pallas_call(
        expert_kernel,
        out_shape=jax.ShapeDtypeStruct((count, width), kind),
        grid=(groups,),
        in_specs=[
            pl.BlockSpec((count, width), lambda g: (0, 0)),
            pl.BlockSpec((1, width, hidden), lambda g: (g, 0, 0)),
            pl.BlockSpec((1, width, hidden), lambda g: (g, 0, 0)),
            pl.BlockSpec((1, hidden, width), lambda g: (g, 0, 0)),
        ],
        out_specs=pl.BlockSpec((count, width), lambda g: (0, 0)),
        scratch_shapes=[pltpu.VMEM((count, width), jnp.float32)],
        cost_estimate=pl.CostEstimate(flops=groups * count * width * hidden * 6, bytes_accessed=groups * width * hidden * 6, transcendentals=groups * count * hidden),
        compiler_params=pltpu.CompilerParams(vmem_limit_bytes=60 * 1024 * 1024),
        name=name,
    )(rows, gate, up, down)


def send(source, target, send_sem, recv_sem, peer):
    copy = pltpu.make_async_remote_copy(
        src_ref=source, dst_ref=target, send_sem=send_sem, recv_sem=recv_sem, device_id=peer, device_id_type=MESH
    )
    copy.start()
    return copy


def greet(peers):
    barrier = pltpu.get_barrier_semaphore()
    for peer in peers:
        pl.semaphore_signal(barrier, inc=1, device_id=peer, device_id_type=MESH)
    pl.semaphore_wait(barrier, len(peers))


class Ring:
    def __init__(self, sources, targets, share, sems):
        self.sources, self.targets, self.share = sources, targets, share
        self.send_own, self.recv_own, self.send_on, self.recv_on, self.local = sems
        self.size, self.me = lax.axis_size("tp"), lax.axis_index("tp")
        self.at_right = lax.rem(self.me + 1, self.size)
        self.at_left = lax.rem(self.me + self.size - 1, self.size)
        self.sides = ({"tp": self.at_right}, {"tp": self.at_left})
        self.owners = (self.at_left, self.at_right)
        self.items = range(len(sources))

    def span_of(self, i):
        rows = self.sources[i].shape[0]
        return (rows, 0) if self.share is None else (rows // 2, self.share * (rows // 2))

    def piece(self, ref, i, part):
        rows, start = self.span_of(i)
        return ref.at[pl.ds(start + part * (rows // 2), rows // 2)]

    def whole(self, ref, i):
        rows, start = self.span_of(i)
        return ref.at[pl.ds(start, rows)]

    def start(self):
        self.own, self.onward, self.kept = {}, {}, []
        for order in range(2):
            for i in self.items:
                for side in range(2):
                    part = side if order == 0 else 1 - side
                    self.own[side, order, i] = send(
                        self.piece(self.sources[i], i, part),
                        self.piece(self.targets[i].at[self.me], i, part),
                        self.send_own.at[side, order, i],
                        self.recv_own.at[side, order, i],
                        self.sides[side],
                    )
        for i in self.items:
            copy = pltpu.make_async_copy(self.sources[i], self.targets[i].at[self.me], self.local.at[i])
            copy.start()
            self.kept.append(copy)

    def pass_on(self):
        for i in self.items:
            for side in range(2):
                self.own[side, 0, i].wait_recv()
                view = self.piece(self.targets[i].at[self.owners[side]], i, side)
                self.onward[side, i] = send(
                    view, view, self.send_on.at[side, i], self.recv_on.at[side, i], self.sides[side]
                )

    def finish_sends(self):
        for copy in self.kept:
            copy.wait()
        for i in self.items:
            for side in range(2):
                self.own[side, 0, i].wait_send()
                self.own[side, 1, i].wait_send()
                self.onward[side, i].wait_send()


def ring_sems(count):
    dma = pltpu.SemaphoreType.DMA
    return [dma((2, 2, count)), dma((2, 2, count)), dma((2, count)), dma((2, count)), dma((count,))]


class Spread:
    def __init__(self, sources, targets, x, core, tp_peers, across, other, sems):
        self.sources, self.targets, self.x, self.core = sources, targets, x, core
        self.tp_peers, self.across, self.other = tp_peers, across, other
        self.send_tp, self.recv_tp, self.send_x, self.recv_x, self.send_pair, self.recv_pair, self.local = sems
        self.me, self.size = lax.axis_index("tp"), lax.axis_size("tp")
        self.items = range(len(sources))

    def piece(self, ref, i):
        rows = self.sources[i].shape[0] // (2 * NX)
        return ref.at[pl.ds((self.core * NX + self.x) * rows, rows)]

    def start(self):
        self.first, self.kept = [], []
        for i in self.items:
            for k in range(1, self.size):
                target = self.piece(self.targets[i].at[self.me], i)
                sems = self.send_tp.at[k - 1, i], self.recv_tp.at[k - 1, i]
                self.first.append(send(self.piece(self.sources[i], i), target, *sems, self.tp_peers[k - 1]))
            copy = pltpu.make_async_copy(self.sources[i], self.targets[i].at[self.me], self.local.at[i])
            copy.start()
            self.kept.append(copy)

    def along_x(self):
        self.second = []
        for copy in self.first:
            copy.wait_recv()
        for i in self.items:
            for k in range(1, self.size):
                view = self.piece(self.targets[i].at[lax.rem(self.me + k, self.size)], i)
                for j, peer in enumerate(self.across):
                    sems = self.send_x.at[j, k - 1, i], self.recv_x.at[j, k - 1, i]
                    self.second.append(send(view, view, *sems, peer))

    def to_other(self):
        self.third = []
        for copy in self.second:
            copy.wait_recv()
        for i in self.items:
            rows = self.sources[i].shape[0] // 2
            for k in range(1, self.size):
                owner = lax.rem(self.me + k, self.size)
                view = self.targets[i].at[owner, pl.ds(self.core * rows, rows)]
                sems = self.send_pair.at[k - 1, i], self.recv_pair.at[k - 1, i]
                self.third.append(send(view, view, *sems, self.other))

    def finish(self):
        for copy in self.kept:
            copy.wait()
        for copy in self.third:
            copy.wait_recv()
        for copy in self.first + self.second + self.third:
            copy.wait_send()


def spread_sems(peers, count):
    dma = pltpu.SemaphoreType.DMA
    tp, along = (peers, count), (NX - 1, peers, count)
    return [dma(tp), dma(tp), dma(along), dma(along), dma(tp), dma(tp), dma((count,))]


def attend_kernel(
    up_ref,
    down_ref,
    shared_gate_ref,
    shared_up_ref,
    shared_down_ref,
    low_ref,
    high_ref,
    block_ref,
    lam_ref,
    gain_ref,
    up_out,
    down_out,
    shared_gate_out,
    shared_up_out,
    shared_down_out,
    out_ref,
    kv_ref,
    swapped,
    high_part,
    high_back,
    query,
    maxima,
    totals,
    weighted,
    send_x,
    recv_x,
    send_z,
    recv_z,
    send_pair,
    recv_pair,
    send_query,
    recv_query,
    send_back,
    recv_back,
    block_sem,
    *sems,
):
    count = lax.axis_size("ep")
    depth = count // (2 * NX)
    place = lax.axis_index("ep")
    core = lax.rem(place, 2)
    chip = lax.div(place, 2)
    x, z = lax.rem(chip, NX), lax.div(chip, NX)

    def at(zz, xx, cc):
        return {"ep": (zz * NX + xx) * 2 + cc}

    other = at(z, x, 1 - core)
    mirror = {"ep": count - 1 - place}
    across = [at(z, lax.rem(x + k, NX), core) for k in (1, 3, 2)]
    up, down = at(lax.rem(z + 1, depth), x, core), at(lax.rem(z + depth - 1, depth), x, core)
    ring = Ring((up_ref, down_ref), (up_out, down_out), None, sems[:5])
    opposite = {"tp": lax.rem(ring.me + 2, ring.size)}
    sources = (shared_gate_ref, shared_up_ref, shared_down_ref)
    targets = (shared_gate_out, shared_up_out, shared_down_out)
    tp_peers = (ring.sides[1], opposite, ring.sides[0])
    spread = Spread(sources, targets, x, core, tp_peers, across, other, sems[5:])
    greet(ring.sides + (opposite, other, mirror, up, down) + tuple(across))

    own_view = kv_ref.at[chip, core]
    along_x = [send(block_ref, own_view, send_x.at[k], recv_x.at[k], across[k]) for k in range(3)]
    own_block = pltpu.make_async_copy(block_ref, own_view, block_sem)
    own_block.start()
    asked = send(high_ref, swapped, send_query, recv_query, mirror)
    spread.start()
    ring.start()
    own_block.wait()
    for copy in along_x:
        copy.wait_recv()

    def level(zz, start, size):
        return kv_ref.at[pl.ds(zz * NX + start, size), core]

    pairs, along_z = [], []

    def to_other(zz, start, size, k):
        view = level(zz, start, size)
        pairs.append(send(view, view, send_pair.at[k], recv_pair.at[k], other))

    last = depth // 2
    for s in range(1, last + 1):
        parts = ((0, NX), (0, NX)) if s < last else ((0, NX // 2), (NX // 2, NX // 2))
        steps = []
        for way, peer in enumerate((up, down)):
            zz = lax.rem(z + (depth - s + 1 if way == 0 else s - 1), depth)
            view = level(zz, *parts[way])
            steps.append(send(view, view, send_z.at[s - 1, way], recv_z.at[s - 1, way], peer))
        if s == 1:
            to_other(z, 0, NX, 0)
        for way in range(2):
            steps[way].wait_recv()
            zz = lax.rem(z + (depth - s if way == 0 else s), depth)
            to_other(zz, *parts[way], 2 * s - 1 + way)
        along_z += steps
        if s == 2:
            spread.along_x()
    ring.pass_on()
    spread.to_other()
    for copy in pairs:
        copy.wait_recv()
    asked.wait_recv()

    rows = block_ref.shape[0] // 2
    results = (out_ref, high_part)
    attention(place, count, rows, swapped, low_ref, kv_ref, lam_ref, gain_ref, results, query, maxima, totals, weighted)
    answer = send(high_part, high_back, send_back, recv_back, mirror)

    for copy in along_x + along_z + pairs + [asked, answer]:
        copy.wait_send()
    answer.wait_recv()
    out_ref[rows // 2 :, :] = high_back[...]
    spread.finish()
    for i in ring.items:
        for side in range(2):
            ring.own[side, 1, i].wait_recv()
            ring.onward[side, i].wait_recv()
    ring.finish_sends()


def attend(weights, low, high, block, lambdas, head_gain):
    size = lax.axis_size("tp")
    count = lax.axis_size("ep")
    half = block.shape[0] // 4
    value_dim = head_gain.shape[0]
    lam = jnp.repeat(lambdas, half).reshape(1, 2 * half)
    vmem = pl.BlockSpec(memory_space=pltpu.VMEM)
    hbm = pl.BlockSpec(memory_space=pltpu.HBM)
    dma = pltpu.SemaphoreType.DMA
    steps = count // (4 * NX)
    return pl.pallas_call(
        attend_kernel,
        out_shape=[jax.ShapeDtypeStruct((size,) + w.shape, w.dtype) for w in weights]
        + [jax.ShapeDtypeStruct((2 * half, 2 * value_dim), jnp.bfloat16)],
        in_specs=[hbm] * 5 + [vmem] * 5,
        out_specs=[hbm] * 5 + [vmem],
        scratch_shapes=[
            pltpu.VMEM((count // 2, 2) + block.shape, block.dtype),
            pltpu.VMEM(high.shape, high.dtype),
            pltpu.VMEM((half, 2 * value_dim), jnp.bfloat16),
            pltpu.VMEM((half, 2 * value_dim), jnp.bfloat16),
            pltpu.VMEM((2, 2, 2 * HEAD, 2 * half), jnp.bfloat16),
            pltpu.VMEM((2, 2, 1, 2 * half), jnp.float32),
            pltpu.VMEM((2, 2, 1, 2 * half), jnp.float32),
            pltpu.VMEM((2, 2, value_dim, 2 * half), jnp.float32),
            dma((3,)),
            dma((3,)),
            dma((steps, 2)),
            dma((steps, 2)),
            dma((2 * steps + 1,)),
            dma((2 * steps + 1,)),
            dma,
            dma,
            dma,
            dma,
            dma,
        ]
        + ring_sems(2)
        + spread_sems(size - 1, 3),
        cost_estimate=pl.CostEstimate(flops=0, bytes_accessed=300_000_000, transcendentals=0),
        compiler_params=pltpu.CompilerParams(collective_id=0, has_side_effects=True, vmem_limit_bytes=60 * 1024 * 1024),
        name="attend",
    )(*weights, low, high, block, lam, head_gain.reshape(value_dim, 1))


def body(
    mixer_input,
    mixer_gain,
    query_one,
    query_two,
    key_one,
    key_two,
    value_weight,
    lambdas,
    head_gain,
    output_weight,
    expert_input,
    expert_gain,
    routes,
    route_weight,
    expert_gate,
    expert_up,
    expert_down,
    shared_gate,
    shared_up,
    shared_down,
):
    ep_size = lax.axis_size("ep")
    tp_size = lax.axis_size("tp")
    ep_rank = lax.axis_index("ep")
    mixer_rows, model_width = mixer_input.shape
    half_rows = mixer_rows // 2
    token_rows = expert_input.shape[0]

    gate_all = lax.all_gather(expert_gate[0], "tp")

    normed = normalize(mixer_input, mixer_gain)
    query_cols = query_one.shape[1]
    turned_weight = jnp.concatenate([query_one, query_two, value_weight], axis=1)
    turned = lax.dot_general(turned_weight, normed, (((0,), (1,)), ((), ())), preferred_element_type=jnp.float32)
    keys = jnp.dot(normed, jnp.concatenate([key_one, key_two], axis=1), preferred_element_type=jnp.float32)
    keys = keys.astype(jnp.bfloat16)
    queries = (turned[: 2 * query_cols].astype(jnp.bfloat16) * HEAD ** (-0.5)).astype(jnp.bfloat16)
    values = turned[2 * query_cols :].astype(jnp.bfloat16)
    key_values = jnp.concatenate([keys, values[:, :half_rows], values[:, half_rows:]], axis=0)

    normed_experts = normalize(expert_input, expert_gain)
    expert_count = expert_gate.shape[0] * ep_size
    top_count = routes.shape[1]
    capacity = max(2, 5 * token_rows * top_count // (4 * expert_count))
    slot_count = expert_count * capacity
    flat_routes = routes.reshape(-1)
    onehot = (flat_routes[:, None] == jnp.arange(expert_count, dtype=jnp.int32)[None, :]).astype(jnp.bfloat16)
    before = jnp.tril(jnp.ones((token_rows * top_count, token_rows * top_count), jnp.bfloat16), -1)
    counts = jnp.dot(before, onehot, preferred_element_type=jnp.float32)
    slot_place = jnp.sum(counts * onehot, axis=1).astype(jnp.int32)
    slot_ids = (flat_routes * capacity + slot_place).reshape(token_rows, top_count)
    slot_match = jnp.arange(slot_count, dtype=jnp.int32)[:, None, None] == slot_ids[None, :, :]
    select = jnp.any(slot_match, axis=2).astype(jnp.bfloat16)
    outgoing = jnp.dot(select, normed_experts, preferred_element_type=jnp.float32).astype(jnp.bfloat16)
    lines = slot_count // ep_size * model_width // 128
    outgoing = outgoing.reshape(ep_size, lines, 128)
    received = lax.all_to_all(outgoing, "ep", split_axis=0, concat_axis=0, tiled=True)

    weights = (expert_up[0], expert_down[0], shared_gate, shared_up, shared_down)
    up_all, down_all, *shared_weights, head_rows = attend(
        weights, queries[:, :half_rows], queries[:, half_rows:], key_values, lambdas, head_gain
    )

    slot_rows = received.reshape(slot_count, model_width)
    routed_result = swiglu_groups(slot_rows, gate_all, up_all, down_all, jnp.bfloat16, "routed")
    routed_result = routed_result.reshape(ep_size, lines, 128)

    normed_again, head_rows, routed_result = lax.optimization_barrier((normed_experts, head_rows, routed_result))
    returned = lax.all_to_all(routed_result, "ep", split_axis=0, concat_axis=0, tiled=True)
    shared_result = swiglu_groups(normed_again, *shared_weights, jnp.float32, "shared")
    partial = jnp.dot(head_rows, output_weight, preferred_element_type=jnp.float32).astype(jnp.bfloat16)
    partial = partial.reshape(tp_size, mixer_rows // tp_size, model_width)
    tp_rank = lax.axis_index("tp")
    mixer_sum = lax.dynamic_index_in_dim(partial, tp_rank, 0, keepdims=False).astype(jnp.float32)
    for step in range(1, tp_size):
        leaving = lax.dynamic_index_in_dim(partial, lax.rem(tp_rank + step, tp_size), 0, keepdims=False)
        part = lax.ppermute(leaving, "tp", [(i, (i + step) % tp_size) for i in range(tp_size)])
        mixer_sum = mixer_sum + part.astype(jnp.float32)
    mixer_output = mixer_sum.astype(jnp.bfloat16)

    returned, mixer_output, shared_result = lax.optimization_barrier((returned, mixer_output, shared_result))
    returned = returned.reshape(slot_count, model_width)
    picks = slot_ids[:, :, None] == jnp.arange(slot_count, dtype=jnp.int32)[None, None, :]
    picks = picks.astype(jnp.bfloat16)
    routed_total = jnp.zeros((token_rows, model_width), jnp.float32)
    for k in range(top_count):
        picked = jnp.dot(picks[:, k], returned, preferred_element_type=jnp.float32)
        routed_total = routed_total + picked * route_weight[:, k : k + 1]
    expert_output = (routed_total + shared_result).astype(jnp.bfloat16)
    return (mixer_output, expert_output)


def solution(mesh):
    in_specs = (
        P("ep", None),
        P(),
        P(None, "tp"),
        P(None, "tp"),
        P(None, "tp"),
        P(None, "tp"),
        P(None, "tp"),
        P("tp"),
        P(),
        P("tp", None),
        P(("ep", "tp"), None),
        P(),
        P(("ep", "tp"), None),
        P(("ep", "tp"), None),
        P("ep", None, "tp"),
        P("ep", None, "tp"),
        P("ep", "tp", None),
        P(None, "tp"),
        P(None, "tp"),
        P("tp", None),
    )
    out_specs = (P(("ep", "tp"), None), P(("ep", "tp"), None))
    return jax.shard_map(body, mesh=mesh, in_specs=in_specs, out_specs=out_specs, check_vma=False)
```

```python
import jax
import jax.numpy as jnp
from jax import lax
from jax.experimental import pallas as pl
from jax.experimental.pallas import tpu as pltpu
from jax.sharding import PartitionSpec as P

HEAD = 64

EPS = 1e-06
NEG = -1e30
MESH = pl.DeviceIdType.MESH

SPAN = 2
NX = 4


def normalize(activations, scaling):
    values = activations.astype(jnp.float32)
    factor = lax.rsqrt(jnp.mean(values * values, axis=-1, keepdims=True) + EPS)
    return (values * factor * scaling).astype(jnp.bfloat16)


def attention(rank, shards, rows, high_ref, low_ref, kv_ref, lam_ref, gain_ref, results, query, maxima, totals, weighted):
    half = rows // 2
    span_keys = SPAN * rows
    zeros = jnp.zeros((HEAD, 2 * half), jnp.bfloat16)
    for which, source in enumerate((low_ref, high_ref)):
        first = jnp.concatenate([source[0:HEAD], source[HEAD : 2 * HEAD]], axis=1)
        second = jnp.concatenate([source[2 * HEAD : 3 * HEAD], source[3 * HEAD : 4 * HEAD]], axis=1)
        query[which, 0, 0:HEAD] = first
        query[which, 0, HEAD : 2 * HEAD] = zeros
        query[which, 1, 0:HEAD] = zeros
        query[which, 1, HEAD : 2 * HEAD] = second

    def block(which, chip, masked, query_start):
        keys = kv_ref[chip, :, 0:rows, :].reshape(span_keys, 2 * HEAD)
        values = [kv_ref[chip, i, rows + j * half : rows + (j + 1) * half, :] for i in range(SPAN) for j in range(2)]
        values = jnp.concatenate(values, axis=1)
        if masked:
            key_pos = chip * span_keys + lax.broadcasted_iota(jnp.int32, (span_keys, 2 * half), 0)
            lane = lax.broadcasted_iota(jnp.int32, (span_keys, 2 * half), 1)
            query_pos = query_start + jnp.where(lane >= half, lane - half, lane)
            visible = key_pos <= query_pos
        for m in range(2):
            scores = jnp.dot(keys, query[which, m], preferred_element_type=jnp.float32)
            if masked:
                scores = jnp.where(visible, scores, NEG)
            earlier = maxima[which, m]
            latest = jnp.maximum(earlier, jnp.max(scores, axis=0, keepdims=True))
            shrink = jnp.exp(earlier - latest)
            weights = jnp.exp(scores - latest)
            if masked:
                weights = jnp.where(visible, weights, 0.0)
            totals[which, m] = totals[which, m] * shrink + jnp.sum(weights, axis=0, keepdims=True)
            product = jnp.dot(values, weights.astype(jnp.bfloat16), preferred_element_type=jnp.float32)
            weighted[which, m] = weighted[which, m] * shrink + product
            maxima[which, m] = latest

    for which in (1, 0):
        maxima[which] = jnp.full(maxima.shape[1:], NEG, jnp.float32)
        totals[which] = jnp.zeros(totals.shape[1:], jnp.float32)
        weighted[which] = jnp.zeros(weighted.shape[1:], jnp.float32)
        full = rank if which == 0 else shards - 1 - rank
        steps = full // SPAN

        def step(i, carry, which=which):
            block(which, i, False, 0)
            return carry

        lax.fori_loop(0, steps, step, 0)
        block(which, steps, True, full * rows + which * half)
        mixed = [weighted[which, m] / totals[which, m] for m in range(2)]
        combined = mixed[0] - lam_ref[...] * mixed[1]
        factor = lax.rsqrt(jnp.mean(combined * combined, axis=0, keepdims=True) + EPS)
        normed = combined * factor * gain_ref[...]
        for head in range(2):
            part = normed[:, head * half : (head + 1) * half]
            results[which][0:half, head * 128 : (head + 1) * 128] = part.T.astype(jnp.bfloat16)


def expert_kernel(rows_ref, gate_ref, up_ref, down_ref, out_ref, total):
    group = pl.program_id(0)
    rows = rows_ref[...]
    gated = jnp.dot(rows, gate_ref[0], preferred_element_type=jnp.float32)
    lifted = jnp.dot(rows, up_ref[0], preferred_element_type=jnp.float32)
    hidden = (gated / (1.0 + jnp.exp(-gated)) * lifted).astype(jnp.bfloat16)
    part = jnp.dot(hidden, down_ref[0], preferred_element_type=jnp.float32)
    part = part.astype(jnp.bfloat16).astype(jnp.float32)

    @pl.when(group == 0)
    def _():
        total[...] = part

    @pl.when(group > 0)
    def _():
        total[...] += part

    @pl.when(group == pl.num_programs(0) - 1)
    def _():
        out_ref[...] = total[...].astype(out_ref.dtype)


def swiglu_groups(rows, gate, up, down, kind, name):
    groups, width, hidden = gate.shape
    count = rows.shape[0]
    return pl.pallas_call(
        expert_kernel,
        out_shape=jax.ShapeDtypeStruct((count, width), kind),
        grid=(groups,),
        in_specs=[
            pl.BlockSpec((count, width), lambda g: (0, 0)),
            pl.BlockSpec((1, width, hidden), lambda g: (g, 0, 0)),
            pl.BlockSpec((1, width, hidden), lambda g: (g, 0, 0)),
            pl.BlockSpec((1, hidden, width), lambda g: (g, 0, 0)),
        ],
        out_specs=pl.BlockSpec((count, width), lambda g: (0, 0)),
        scratch_shapes=[pltpu.VMEM((count, width), jnp.float32)],
        cost_estimate=pl.CostEstimate(flops=groups * count * width * hidden * 6, bytes_accessed=groups * width * hidden * 6, transcendentals=groups * count * hidden),
        compiler_params=pltpu.CompilerParams(vmem_limit_bytes=60 * 1024 * 1024),
        name=name,
    )(rows, gate, up, down)


def send(source, target, send_sem, recv_sem, peer):
    copy = pltpu.make_async_remote_copy(
        src_ref=source, dst_ref=target, send_sem=send_sem, recv_sem=recv_sem, device_id=peer, device_id_type=MESH
    )
    copy.start()
    return copy


def greet(peers, count):
    barrier = pltpu.get_barrier_semaphore()
    place = lax.axis_index("ep")
    for peer in peers:
        pl.semaphore_signal(barrier, inc=1, device_id=peer, device_id_type=MESH)

    def one(k, carry):
        peer = {"ep": lax.rem(place + k, count)}
        pl.semaphore_signal(barrier, inc=1, device_id=peer, device_id_type=MESH)
        return carry

    lax.fori_loop(1, count, one, 0)
    pl.semaphore_wait(barrier, len(peers) + count - 1)


class Ring:
    def __init__(self, sources, targets, share, sems):
        self.sources, self.targets, self.share = sources, targets, share
        self.send_own, self.recv_own, self.send_on, self.recv_on, self.local = sems
        self.size, self.me = lax.axis_size("tp"), lax.axis_index("tp")
        self.at_right = lax.rem(self.me + 1, self.size)
        self.at_left = lax.rem(self.me + self.size - 1, self.size)
        self.sides = ({"tp": self.at_right}, {"tp": self.at_left})
        self.owners = (self.at_left, self.at_right)
        self.items = range(len(sources))

    def span_of(self, i):
        rows = self.sources[i].shape[0]
        return (rows, 0) if self.share is None else (rows // 2, self.share * (rows // 2))

    def piece(self, ref, i, part):
        rows, start = self.span_of(i)
        return ref.at[pl.ds(start + part * (rows // 2), rows // 2)]

    def whole(self, ref, i):
        rows, start = self.span_of(i)
        return ref.at[pl.ds(start, rows)]

    def start(self):
        self.own, self.onward, self.kept = {}, {}, []
        for order in range(2):
            for i in self.items:
                for side in range(2):
                    part = side if order == 0 else 1 - side
                    self.own[side, order, i] = send(
                        self.piece(self.sources[i], i, part),
                        self.piece(self.targets[i].at[self.me], i, part),
                        self.send_own.at[side, order, i],
                        self.recv_own.at[side, order, i],
                        self.sides[side],
                    )
        for i in self.items:
            copy = pltpu.make_async_copy(self.sources[i], self.targets[i].at[self.me], self.local.at[i])
            copy.start()
            self.kept.append(copy)

    def pass_on(self):
        for i in self.items:
            for side in range(2):
                self.own[side, 0, i].wait_recv()
                view = self.piece(self.targets[i].at[self.owners[side]], i, side)
                self.onward[side, i] = send(
                    view, view, self.send_on.at[side, i], self.recv_on.at[side, i], self.sides[side]
                )

    def finish_sends(self):
        for i in self.items:
            for side in range(2):
                self.own[side, 0, i].wait_send()
                self.own[side, 1, i].wait_send()
                self.onward[side, i].wait_send()


def ring_sems(count):
    dma = pltpu.SemaphoreType.DMA
    return [dma((2, 2, count)), dma((2, 2, count)), dma((2, count)), dma((2, count)), dma((count,))]


class Spread:
    def __init__(self, sources, targets, x, core, tp_peers, across, other, sems):
        self.sources, self.targets, self.x, self.core = sources, targets, x, core
        self.tp_peers, self.across, self.other = tp_peers, across, other
        self.send_tp, self.recv_tp, self.send_x, self.recv_x, self.send_pair, self.recv_pair, self.local = sems
        self.me, self.size = lax.axis_index("tp"), lax.axis_size("tp")
        self.items = range(len(sources))

    def piece(self, ref, i):
        rows = self.sources[i].shape[0] // (2 * NX)
        return ref.at[pl.ds((self.core * NX + self.x) * rows, rows)]

    def start(self):
        self.first, self.kept = [], []
        for i in self.items:
            for k in range(1, self.size):
                target = self.piece(self.targets[i].at[self.me], i)
                sems = self.send_tp.at[k - 1, i], self.recv_tp.at[k - 1, i]
                self.first.append(send(self.piece(self.sources[i], i), target, *sems, self.tp_peers[k - 1]))
            copy = pltpu.make_async_copy(self.sources[i], self.targets[i].at[self.me], self.local.at[i])
            copy.start()
            self.kept.append(copy)

    def along_x(self):
        self.second = []
        for copy in self.first:
            copy.wait_recv()
        for i in self.items:
            for k in range(1, self.size):
                view = self.piece(self.targets[i].at[lax.rem(self.me + k, self.size)], i)
                for j, peer in enumerate(self.across):
                    sems = self.send_x.at[j, k - 1, i], self.recv_x.at[j, k - 1, i]
                    self.second.append(send(view, view, *sems, peer))

    def to_other(self):
        self.third = []
        for copy in self.second:
            copy.wait_recv()
        for i in self.items:
            rows = self.sources[i].shape[0] // 2
            for k in range(1, self.size):
                owner = lax.rem(self.me + k, self.size)
                view = self.targets[i].at[owner, pl.ds(self.core * rows, rows)]
                sems = self.send_pair.at[k - 1, i], self.recv_pair.at[k - 1, i]
                self.third.append(send(view, view, *sems, self.other))

    def finish(self):
        for copy in self.kept:
            copy.wait()
        for copy in self.third:
            copy.wait_recv()
        for copy in self.first + self.second + self.third:
            copy.wait_send()


def spread_sems(peers, count):
    dma = pltpu.SemaphoreType.DMA
    tp, along = (peers, count), (NX - 1, peers, count)
    return [dma(tp), dma(tp), dma(along), dma(along), dma(tp), dma(tp), dma((count,))]


def attend_kernel(
    gate_ref,
    up_ref,
    down_ref,
    shared_gate_ref,
    shared_up_ref,
    shared_down_ref,
    leaving_ref,
    low_ref,
    high_ref,
    block_ref,
    lam_ref,
    gain_ref,
    shared_gate_out,
    shared_up_out,
    shared_down_out,
    landed_ref,
    routed_ref,
    out_ref,
    gate_all,
    up_all,
    down_all,
    landed,
    total,
    kv_ref,
    swapped,
    high_part,
    high_back,
    query,
    maxima,
    totals,
    weighted,
    send_x,
    recv_x,
    send_z,
    recv_z,
    send_pair,
    recv_pair,
    send_query,
    recv_query,
    send_back,
    recv_back,
    send_rows,
    recv_rows,
    block_sem,
    *sems,
):
    count = lax.axis_size("ep")
    depth = count // (2 * NX)
    place = lax.axis_index("ep")
    core = lax.rem(place, 2)
    chip = lax.div(place, 2)
    x, z = lax.rem(chip, NX), lax.div(chip, NX)

    def at(zz, xx, cc):
        return {"ep": (zz * NX + xx) * 2 + cc}

    other = at(z, x, 1 - core)
    mirror = {"ep": count - 1 - place}
    across = [at(z, lax.rem(x + k, NX), core) for k in (1, 3, 2)]
    up, down = at(lax.rem(z + 1, depth), x, core), at(lax.rem(z + depth - 1, depth), x, core)
    ring = Ring((gate_ref, up_ref, down_ref), (gate_all, up_all, down_all), None, sems[:5])
    opposite = {"tp": lax.rem(ring.me + 2, ring.size)}
    sources = (shared_gate_ref, shared_up_ref, shared_down_ref)
    targets = (shared_gate_out, shared_up_out, shared_down_out)
    tp_peers = (ring.sides[1], opposite, ring.sides[0])
    spread = Spread(sources, targets, x, core, tp_peers, across, other, sems[5:])
    greet(ring.sides + (opposite,), count)

    own_view = kv_ref.at[chip, core]
    along_x = [send(block_ref, own_view, send_x.at[k], recv_x.at[k], across[k]) for k in range(3)]
    own_block = pltpu.make_async_copy(block_ref, own_view, block_sem)
    own_block.start()
    asked = send(high_ref, swapped, send_query, recv_query, mirror)
    spread.start()
    ring.start()
    own_block.wait()
    for copy in along_x:
        copy.wait_recv()

    def level(zz, start, size):
        return kv_ref.at[pl.ds(zz * NX + start, size), core]

    pairs, along_z = [], []

    def to_other(zz, start, size, k):
        view = level(zz, start, size)
        pairs.append(send(view, view, send_pair.at[k], recv_pair.at[k], other))

    last = depth // 2
    for s in range(1, last + 1):
        parts = ((0, NX), (0, NX)) if s < last else ((0, NX // 2), (NX // 2, NX // 2))
        steps = []
        for way, peer in enumerate((up, down)):
            zz = lax.rem(z + (depth - s + 1 if way == 0 else s - 1), depth)
            view = level(zz, *parts[way])
            steps.append(send(view, view, send_z.at[s - 1, way], recv_z.at[s - 1, way], peer))
        if s == 1:
            to_other(z, 0, NX, 0)
        for way in range(2):
            steps[way].wait_recv()
            zz = lax.rem(z + (depth - s if way == 0 else s), depth)
            to_other(zz, *parts[way], 2 * s - 1 + way)
        along_z += steps
        if s == 2:
            spread.along_x()
    ring.pass_on()

    slots = leaving_ref.shape[0] // count

    def rows_of(ref, owner):
        return ref.at[pl.ds(pl.multiple_of(owner * slots, slots), slots)]

    def row_copy(k):
        peer = lax.rem(place + k, count)
        return pltpu.make_async_remote_copy(
            src_ref=rows_of(leaving_ref, peer),
            dst_ref=rows_of(landed_ref, place),
            send_sem=send_rows.at[k],
            recv_sem=recv_rows.at[k],
            device_id={"ep": peer},
            device_id_type=MESH,
        )

    def start_rows(k, carry):
        row_copy(k).start()
        return carry

    def wait_rows(k, carry):
        row_copy(k).wait()
        return carry

    lax.fori_loop(1, count, start_rows, 0)
    own_rows = pltpu.make_async_copy(rows_of(leaving_ref, place), rows_of(landed_ref, place), send_rows.at[0])
    own_rows.start()
    spread.to_other()
    for copy in pairs:
        copy.wait_recv()
    asked.wait_recv()

    rows = block_ref.shape[0] // 2
    results = (out_ref, high_part)
    attention(place, count, rows, swapped, low_ref, kv_ref, lam_ref, gain_ref, results, query, maxima, totals, weighted)
    answer = send(high_part, high_back, send_back, recv_back, mirror)

    lax.fori_loop(1, count, wait_rows, 0)
    own_rows.wait()
    fetch = pltpu.make_async_copy(landed_ref, landed, recv_rows.at[0])
    fetch.start()
    for copy in along_x + along_z + pairs + [asked, answer]:
        copy.wait_send()
    answer.wait_recv()
    out_ref[rows // 2 :, :] = high_back[...]
    fetch.wait()

    def group(owner, first):
        tile = 256

        def step(i, carry):
            span = pl.ds(pl.multiple_of(i * tile, tile), tile)
            some = landed[span, :]
            gated = jnp.dot(some, gate_all[owner], preferred_element_type=jnp.float32)
            lifted = jnp.dot(some, up_all[owner], preferred_element_type=jnp.float32)
            hidden = (gated / (1.0 + jnp.exp(-gated)) * lifted).astype(jnp.bfloat16)
            part = jnp.dot(hidden, down_all[owner], preferred_element_type=jnp.float32)
            part = part.astype(jnp.bfloat16).astype(jnp.float32)
            total[span, :] = part if first else total[span, :] + part
            return carry

        lax.fori_loop(0, landed.shape[0] // tile, step, 0)

    for copy in ring.kept:
        copy.wait()
    group(ring.me, True)
    for side in range(2):
        for i in ring.items:
            ring.own[side, 1, i].wait_recv()
        group(ring.owners[side], False)
    spread.finish()
    for i in ring.items:
        for side in range(2):
            ring.onward[side, i].wait_recv()
    group(lax.rem(ring.me + 2, ring.size), False)
    routed_ref[...] = total[...].astype(routed_ref.dtype)
    ring.finish_sends()


def attend(weights, leaving, low, high, block, lambdas, head_gain):
    size = lax.axis_size("tp")
    count = lax.axis_size("ep")
    half = block.shape[0] // 4
    value_dim = head_gain.shape[0]
    lam = jnp.repeat(lambdas, half).reshape(1, 2 * half)
    vmem = pl.BlockSpec(memory_space=pltpu.VMEM)
    hbm = pl.BlockSpec(memory_space=pltpu.HBM)
    dma = pltpu.SemaphoreType.DMA
    steps = count // (4 * NX)
    return pl.pallas_call(
        attend_kernel,
        out_shape=[jax.ShapeDtypeStruct((size,) + w.shape, w.dtype) for w in weights[3:]]
        + [jax.ShapeDtypeStruct(leaving.shape, leaving.dtype)] * 2
        + [jax.ShapeDtypeStruct((2 * half, 2 * value_dim), jnp.bfloat16)],
        in_specs=[hbm] * 7 + [vmem] * 5,
        out_specs=[hbm] * 4 + [vmem] * 2,
        scratch_shapes=[pltpu.VMEM((size,) + w.shape, w.dtype) for w in weights[:3]]
        + [
            pltpu.VMEM(leaving.shape, leaving.dtype),
            pltpu.VMEM(leaving.shape, jnp.float32),
            pltpu.VMEM((count // 2, 2) + block.shape, block.dtype),
            pltpu.VMEM(high.shape, high.dtype),
            pltpu.VMEM((half, 2 * value_dim), jnp.bfloat16),
            pltpu.VMEM((half, 2 * value_dim), jnp.bfloat16),
            pltpu.VMEM((2, 2, 2 * HEAD, 2 * half), jnp.bfloat16),
            pltpu.VMEM((2, 2, 1, 2 * half), jnp.float32),
            pltpu.VMEM((2, 2, 1, 2 * half), jnp.float32),
            pltpu.VMEM((2, 2, value_dim, 2 * half), jnp.float32),
            dma((3,)),
            dma((3,)),
            dma((steps, 2)),
            dma((steps, 2)),
            dma((2 * steps + 1,)),
            dma((2 * steps + 1,)),
            dma,
            dma,
            dma,
            dma,
            dma((count,)),
            dma((count,)),
            dma,
        ]
        + ring_sems(3)
        + spread_sems(size - 1, 3),
        cost_estimate=pl.CostEstimate(flops=0, bytes_accessed=300_000_000, transcendentals=0),
        compiler_params=pltpu.CompilerParams(collective_id=0, has_side_effects=True, vmem_limit_bytes=60 * 1024 * 1024),
        name="attend",
    )(*weights, leaving, low, high, block, lam, head_gain.reshape(value_dim, 1))


def body(
    mixer_input,
    mixer_gain,
    query_one,
    query_two,
    key_one,
    key_two,
    value_weight,
    lambdas,
    head_gain,
    output_weight,
    expert_input,
    expert_gain,
    routes,
    route_weight,
    expert_gate,
    expert_up,
    expert_down,
    shared_gate,
    shared_up,
    shared_down,
):
    ep_size = lax.axis_size("ep")
    tp_size = lax.axis_size("tp")
    ep_rank = lax.axis_index("ep")
    mixer_rows, model_width = mixer_input.shape
    half_rows = mixer_rows // 2
    token_rows = expert_input.shape[0]

    normed = normalize(mixer_input, mixer_gain)
    query_cols = query_one.shape[1]
    turned_weight = jnp.concatenate([query_one, query_two, value_weight], axis=1)
    turned = lax.dot_general(turned_weight, normed, (((0,), (1,)), ((), ())), preferred_element_type=jnp.float32)
    keys = jnp.dot(normed, jnp.concatenate([key_one, key_two], axis=1), preferred_element_type=jnp.float32)
    keys = keys.astype(jnp.bfloat16)
    queries = (turned[: 2 * query_cols].astype(jnp.bfloat16) * HEAD ** (-0.5)).astype(jnp.bfloat16)
    values = turned[2 * query_cols :].astype(jnp.bfloat16)
    key_values = jnp.concatenate([keys, values[:, :half_rows], values[:, half_rows:]], axis=0)

    normed_experts = normalize(expert_input, expert_gain)
    expert_count = expert_gate.shape[0] * ep_size
    top_count = routes.shape[1]
    capacity = max(2, 5 * token_rows * top_count // (4 * expert_count))
    slot_count = expert_count * capacity
    flat_routes = routes.reshape(-1)
    onehot = (flat_routes[:, None] == jnp.arange(expert_count, dtype=jnp.int32)[None, :]).astype(jnp.bfloat16)
    before = jnp.tril(jnp.ones((token_rows * top_count, token_rows * top_count), jnp.bfloat16), -1)
    counts = jnp.dot(before, onehot, preferred_element_type=jnp.float32)
    slot_place = jnp.sum(counts * onehot, axis=1).astype(jnp.int32)
    slot_ids = (flat_routes * capacity + slot_place).reshape(token_rows, top_count)
    padded = -(-capacity // 8) * 8
    leaving_ids = (flat_routes * padded + slot_place).reshape(token_rows, top_count)
    slot_match = jnp.arange(expert_count * padded, dtype=jnp.int32)[:, None, None] == leaving_ids[None, :, :]
    select = jnp.any(slot_match, axis=2).astype(jnp.bfloat16)
    outgoing = jnp.dot(select, normed_experts, preferred_element_type=jnp.float32).astype(jnp.bfloat16)

    weights = (expert_gate[0], expert_up[0], expert_down[0], shared_gate, shared_up, shared_down)
    *shared_weights, _, routed_result, head_rows = attend(
        weights, outgoing, queries[:, :half_rows], queries[:, half_rows:], key_values, lambdas, head_gain
    )
    lines = slot_count // ep_size * model_width // 128
    routed_result = routed_result.reshape(ep_size, padded, model_width)[:, :capacity].reshape(ep_size, lines, 128)

    normed_again, head_rows, routed_result = lax.optimization_barrier((normed_experts, head_rows, routed_result))
    returned = lax.all_to_all(routed_result, "ep", split_axis=0, concat_axis=0, tiled=True)
    shared_result = swiglu_groups(normed_again, *shared_weights, jnp.float32, "shared")
    partial = jnp.dot(head_rows, output_weight, preferred_element_type=jnp.float32).astype(jnp.bfloat16)
    partial = partial.reshape(tp_size, mixer_rows // tp_size, model_width)
    tp_rank = lax.axis_index("tp")
    mixer_sum = lax.dynamic_index_in_dim(partial, tp_rank, 0, keepdims=False).astype(jnp.float32)
    for step in range(1, tp_size):
        leaving = lax.dynamic_index_in_dim(partial, lax.rem(tp_rank + step, tp_size), 0, keepdims=False)
        part = lax.ppermute(leaving, "tp", [(i, (i + step) % tp_size) for i in range(tp_size)])
        mixer_sum = mixer_sum + part.astype(jnp.float32)
    mixer_output = mixer_sum.astype(jnp.bfloat16)

    returned, mixer_output, shared_result = lax.optimization_barrier((returned, mixer_output, shared_result))
    returned = returned.reshape(slot_count, model_width)
    picks = slot_ids[:, :, None] == jnp.arange(slot_count, dtype=jnp.int32)[None, None, :]
    picks = picks.astype(jnp.bfloat16)
    routed_total = jnp.zeros((token_rows, model_width), jnp.float32)
    for k in range(top_count):
        picked = jnp.dot(picks[:, k], returned, preferred_element_type=jnp.float32)
        routed_total = routed_total + picked * route_weight[:, k : k + 1]
    expert_output = (routed_total + shared_result).astype(jnp.bfloat16)
    return (mixer_output, expert_output)


def solution(mesh):
    in_specs = (
        P("ep", None),
        P(),
        P(None, "tp"),
        P(None, "tp"),
        P(None, "tp"),
        P(None, "tp"),
        P(None, "tp"),
        P("tp"),
        P(),
        P("tp", None),
        P(("ep", "tp"), None),
        P(),
        P(("ep", "tp"), None),
        P(("ep", "tp"), None),
        P("ep", None, "tp"),
        P("ep", None, "tp"),
        P("ep", "tp", None),
        P(None, "tp"),
        P(None, "tp"),
        P("tp", None),
    )
    out_specs = (P(("ep", "tp"), None), P(("ep", "tp"), None))
    return jax.shard_map(body, mesh=mesh, in_specs=in_specs, out_specs=out_specs, check_vma=False)
```

```python
import jax
import jax.numpy as jnp
from jax import lax
from jax.experimental import pallas as pl
from jax.experimental.pallas import tpu as pltpu
from jax.sharding import PartitionSpec as P

HEAD = 64

EPS = 1e-06
NEG = -1e30
MESH = pl.DeviceIdType.MESH

SPAN = 2
NX = 4


def normalize(activations, scaling):
    values = activations.astype(jnp.float32)
    factor = lax.rsqrt(jnp.mean(values * values, axis=-1, keepdims=True) + EPS)
    return (values * factor * scaling).astype(jnp.bfloat16)


def attention(rank, shards, rows, high_ref, low_ref, kv_ref, lam_ref, gain_ref, results, query, maxima, totals, weighted):
    half = rows // 2
    span_keys = SPAN * rows
    zeros = jnp.zeros((HEAD, 2 * half), jnp.bfloat16)
    for which, source in enumerate((low_ref, high_ref)):
        first = jnp.concatenate([source[0:HEAD], source[HEAD : 2 * HEAD]], axis=1)
        second = jnp.concatenate([source[2 * HEAD : 3 * HEAD], source[3 * HEAD : 4 * HEAD]], axis=1)
        query[which, 0, 0:HEAD] = first
        query[which, 0, HEAD : 2 * HEAD] = zeros
        query[which, 1, 0:HEAD] = zeros
        query[which, 1, HEAD : 2 * HEAD] = second

    def block(which, chip, masked, query_start):
        keys = kv_ref[chip, :, 0:rows, :].reshape(span_keys, 2 * HEAD)
        values = [kv_ref[chip, i, rows + j * half : rows + (j + 1) * half, :] for i in range(SPAN) for j in range(2)]
        values = jnp.concatenate(values, axis=1)
        if masked:
            key_pos = chip * span_keys + lax.broadcasted_iota(jnp.int32, (span_keys, 2 * half), 0)
            lane = lax.broadcasted_iota(jnp.int32, (span_keys, 2 * half), 1)
            query_pos = query_start + jnp.where(lane >= half, lane - half, lane)
            visible = key_pos <= query_pos
        for m in range(2):
            scores = jnp.dot(keys, query[which, m], preferred_element_type=jnp.float32)
            if masked:
                scores = jnp.where(visible, scores, NEG)
            earlier = maxima[which, m]
            latest = jnp.maximum(earlier, jnp.max(scores, axis=0, keepdims=True))
            shrink = jnp.exp(earlier - latest)
            weights = jnp.exp(scores - latest)
            if masked:
                weights = jnp.where(visible, weights, 0.0)
            totals[which, m] = totals[which, m] * shrink + jnp.sum(weights, axis=0, keepdims=True)
            product = jnp.dot(values, weights.astype(jnp.bfloat16), preferred_element_type=jnp.float32)
            weighted[which, m] = weighted[which, m] * shrink + product
            maxima[which, m] = latest

    for which in (1, 0):
        maxima[which] = jnp.full(maxima.shape[1:], NEG, jnp.float32)
        totals[which] = jnp.zeros(totals.shape[1:], jnp.float32)
        weighted[which] = jnp.zeros(weighted.shape[1:], jnp.float32)
        full = rank if which == 0 else shards - 1 - rank
        steps = full // SPAN

        def step(i, carry, which=which):
            block(which, i, False, 0)
            return carry

        lax.fori_loop(0, steps, step, 0)
        block(which, steps, True, full * rows + which * half)
        mixed = [weighted[which, m] / totals[which, m] for m in range(2)]
        lane = lax.broadcasted_iota(jnp.int32, (1, 2 * half), 1)
        combined = mixed[0] - jnp.where(lane < half, lam_ref[0], lam_ref[1]) * mixed[1]
        factor = lax.rsqrt(jnp.mean(combined * combined, axis=0, keepdims=True) + EPS)
        normed = combined * factor
        for head in range(2):
            part = normed[:, head * half : (head + 1) * half]
            results[which][0:half, head * 128 : (head + 1) * 128] = (part.T * gain_ref[...]).astype(jnp.bfloat16)


def expert_kernel(rows_ref, gate_ref, up_ref, down_ref, out_ref, total):
    group = pl.program_id(0)
    rows = rows_ref[...]
    gated = jnp.dot(rows, gate_ref[0], preferred_element_type=jnp.float32)
    lifted = jnp.dot(rows, up_ref[0], preferred_element_type=jnp.float32)
    hidden = (gated / (1.0 + jnp.exp(-gated)) * lifted).astype(jnp.bfloat16)
    part = jnp.dot(hidden, down_ref[0], preferred_element_type=jnp.float32)
    part = part.astype(jnp.bfloat16).astype(jnp.float32)

    @pl.when(group == 0)
    def _():
        total[...] = part

    @pl.when(group > 0)
    def _():
        total[...] += part

    @pl.when(group == pl.num_programs(0) - 1)
    def _():
        out_ref[...] = total[...].astype(out_ref.dtype)


def swiglu_groups(rows, gate, up, down, kind, name):
    groups, width, hidden = gate.shape
    count = rows.shape[0]
    return pl.pallas_call(
        expert_kernel,
        out_shape=jax.ShapeDtypeStruct((count, width), kind),
        grid=(groups,),
        in_specs=[
            pl.BlockSpec((count, width), lambda g: (0, 0)),
            pl.BlockSpec((1, width, hidden), lambda g: (g, 0, 0)),
            pl.BlockSpec((1, width, hidden), lambda g: (g, 0, 0)),
            pl.BlockSpec((1, hidden, width), lambda g: (g, 0, 0)),
        ],
        out_specs=pl.BlockSpec((count, width), lambda g: (0, 0)),
        scratch_shapes=[pltpu.VMEM((count, width), jnp.float32)],
        cost_estimate=pl.CostEstimate(flops=groups * count * width * hidden * 6, bytes_accessed=groups * width * hidden * 6, transcendentals=groups * count * hidden),
        compiler_params=pltpu.CompilerParams(vmem_limit_bytes=60 * 1024 * 1024),
        name=name,
    )(rows, gate, up, down)


def send(source, target, send_sem, recv_sem, peer):
    copy = pltpu.make_async_remote_copy(
        src_ref=source, dst_ref=target, send_sem=send_sem, recv_sem=recv_sem, device_id=peer, device_id_type=MESH
    )
    copy.start()
    return copy


def greet(peers, count):
    barrier = pltpu.get_barrier_semaphore()
    place = lax.axis_index("ep")
    for peer in peers:
        pl.semaphore_signal(barrier, inc=1, device_id=peer, device_id_type=MESH)

    def one(k, carry):
        peer = {"ep": lax.rem(place + k, count)}
        pl.semaphore_signal(barrier, inc=1, device_id=peer, device_id_type=MESH)
        return carry

    lax.fori_loop(1, count, one, 0)
    pl.semaphore_wait(barrier, len(peers) + count - 1)


class Ring:
    def __init__(self, sources, targets, share, sems):
        self.sources, self.targets, self.share = sources, targets, share
        self.send_own, self.recv_own, self.send_on, self.recv_on, self.local = sems
        self.size, self.me = lax.axis_size("tp"), lax.axis_index("tp")
        self.at_right = lax.rem(self.me + 1, self.size)
        self.at_left = lax.rem(self.me + self.size - 1, self.size)
        self.sides = ({"tp": self.at_right}, {"tp": self.at_left})
        self.owners = (self.at_left, self.at_right)
        self.items = range(len(sources))

    def span_of(self, i):
        rows = self.sources[i].shape[0]
        return (rows, 0) if self.share is None else (rows // 2, self.share * (rows // 2))

    def piece(self, ref, i, part):
        rows, start = self.span_of(i)
        return ref.at[pl.ds(start + part * (rows // 2), rows // 2)]

    def whole(self, ref, i):
        rows, start = self.span_of(i)
        return ref.at[pl.ds(start, rows)]

    def start(self):
        self.own, self.onward, self.kept = {}, {}, []
        for order in range(2):
            for i in self.items:
                for side in range(2):
                    part = side if order == 0 else 1 - side
                    self.own[side, order, i] = send(
                        self.piece(self.sources[i], i, part),
                        self.piece(self.targets[i].at[self.me], i, part),
                        self.send_own.at[side, order, i],
                        self.recv_own.at[side, order, i],
                        self.sides[side],
                    )
        for i in self.items:
            copy = pltpu.make_async_copy(self.sources[i], self.targets[i].at[self.me], self.local.at[i])
            copy.start()
            self.kept.append(copy)

    def pass_on(self):
        for i in self.items:
            for side in range(2):
                self.own[side, 0, i].wait_recv()
                view = self.piece(self.targets[i].at[self.owners[side]], i, side)
                self.onward[side, i] = send(
                    view, view, self.send_on.at[side, i], self.recv_on.at[side, i], self.sides[side]
                )

    def finish_sends(self):
        for i in self.items:
            for side in range(2):
                self.own[side, 0, i].wait_send()
                self.own[side, 1, i].wait_send()
                self.onward[side, i].wait_send()


def ring_sems(count):
    dma = pltpu.SemaphoreType.DMA
    return [dma((2, 2, count)), dma((2, 2, count)), dma((2, count)), dma((2, count)), dma((count,))]


class Spread:
    def __init__(self, sources, targets, x, core, tp_peers, across, other, sems):
        self.sources, self.targets, self.x, self.core = sources, targets, x, core
        self.tp_peers, self.across, self.other = tp_peers, across, other
        self.send_tp, self.recv_tp, self.send_x, self.recv_x, self.send_pair, self.recv_pair, self.local = sems
        self.me, self.size = lax.axis_index("tp"), lax.axis_size("tp")
        self.items = range(len(sources))

    def piece(self, ref, i):
        rows = self.sources[i].shape[0] // (2 * NX)
        return ref.at[pl.ds((self.core * NX + self.x) * rows, rows)]

    def start(self):
        self.first, self.kept = [], []
        for i in self.items:
            for k in range(1, self.size):
                target = self.piece(self.targets[i].at[self.me], i)
                sems = self.send_tp.at[k - 1, i], self.recv_tp.at[k - 1, i]
                self.first.append(send(self.piece(self.sources[i], i), target, *sems, self.tp_peers[k - 1]))
            copy = pltpu.make_async_copy(self.sources[i], self.targets[i].at[self.me], self.local.at[i])
            copy.start()
            self.kept.append(copy)

    def along_x(self):
        self.second = []
        for copy in self.first:
            copy.wait_recv()
        for i in self.items:
            for k in range(1, self.size):
                view = self.piece(self.targets[i].at[lax.rem(self.me + k, self.size)], i)
                for j, peer in enumerate(self.across):
                    sems = self.send_x.at[j, k - 1, i], self.recv_x.at[j, k - 1, i]
                    self.second.append(send(view, view, *sems, peer))

    def to_other(self):
        self.third = []
        for copy in self.second:
            copy.wait_recv()
        for i in self.items:
            rows = self.sources[i].shape[0] // 2
            for k in range(1, self.size):
                owner = lax.rem(self.me + k, self.size)
                view = self.targets[i].at[owner, pl.ds(self.core * rows, rows)]
                sems = self.send_pair.at[k - 1, i], self.recv_pair.at[k - 1, i]
                self.third.append(send(view, view, *sems, self.other))

    def finish(self):
        for copy in self.kept:
            copy.wait()
        for copy in self.third:
            copy.wait_recv()
        for copy in self.first + self.second + self.third:
            copy.wait_send()


def spread_sems(peers, count):
    dma = pltpu.SemaphoreType.DMA
    tp, along = (peers, count), (NX - 1, peers, count)
    return [dma(tp), dma(tp), dma(along), dma(along), dma(tp), dma(tp), dma((count,))]


def attend_kernel(
    gate_ref,
    up_ref,
    down_ref,
    shared_gate_ref,
    shared_up_ref,
    shared_down_ref,
    mixer_ref,
    query_one_ref,
    query_two_ref,
    value_ref,
    key_one_ref,
    key_two_ref,
    expert_ref,
    slot_ref,
    mixer_gain_ref,
    expert_gain_ref,
    lam_ref,
    gain_ref,
    shared_gate_out,
    shared_up_out,
    shared_down_out,
    leaving_ref,
    landed_ref,
    routed_ref,
    out_ref,
    mixer_rows,
    projections,
    key_rows,
    expert_rows,
    low_ref,
    high_ref,
    block_ref,
    load_sem,
    gate_all,
    up_all,
    down_all,
    landed,
    total,
    kv_ref,
    swapped,
    high_part,
    high_back,
    query,
    maxima,
    totals,
    weighted,
    send_x,
    recv_x,
    send_z,
    recv_z,
    send_pair,
    recv_pair,
    send_query,
    recv_query,
    send_back,
    recv_back,
    send_rows,
    recv_rows,
    block_sem,
    *sems,
):
    count = lax.axis_size("ep")
    depth = count // (2 * NX)
    place = lax.axis_index("ep")
    core = lax.rem(place, 2)
    chip = lax.div(place, 2)
    x, z = lax.rem(chip, NX), lax.div(chip, NX)

    def at(zz, xx, cc):
        return {"ep": (zz * NX + xx) * 2 + cc}

    other = at(z, x, 1 - core)
    mirror = {"ep": count - 1 - place}
    across = [at(z, lax.rem(x + k, NX), core) for k in (1, 3, 2)]
    up, down = at(lax.rem(z + 1, depth), x, core), at(lax.rem(z + depth - 1, depth), x, core)
    ring = Ring((gate_ref, up_ref, down_ref), (gate_all, up_all, down_all), None, sems[:5])
    opposite = {"tp": lax.rem(ring.me + 2, ring.size)}
    sources = (shared_gate_ref, shared_up_ref, shared_down_ref)
    targets = (shared_gate_out, shared_up_out, shared_down_out)
    tp_peers = (ring.sides[1], opposite, ring.sides[0])
    spread = Spread(sources, targets, x, core, tp_peers, across, other, sems[5:])
    loads = [(mixer_ref, mixer_rows), (expert_ref, expert_rows)]
    loads += [(w, projections.at[i]) for i, w in enumerate((query_one_ref, query_two_ref, value_ref))]
    loads += [(w, key_rows.at[pl.ds(i * HEAD, HEAD)]) for i, w in enumerate((key_one_ref, key_two_ref))]
    loads = [pltpu.make_async_copy(source, target, load_sem.at[i]) for i, (source, target) in enumerate(loads)]
    for copy in loads:
        copy.start()
    greet(ring.sides + (opposite,), count)
    spread.start()
    ring.start()
    for copy in loads:
        copy.wait()

    half = mixer_rows.shape[0] // 2
    mixer_rows[...] = normalize(mixer_rows[...], mixer_gain_ref[...])
    normed = mixer_rows[...]

    def project(i):
        product = jnp.dot(normed, projections[i], preferred_element_type=jnp.float32)
        return product.astype(jnp.bfloat16)

    def turned(product, scale):
        return (product.astype(jnp.float32).T * scale).astype(jnp.bfloat16)

    keys = lax.dot_general(normed, key_rows[...], (((1,), (1,)), ((), ())), preferred_element_type=jnp.float32)
    block_ref[0 : 2 * half] = keys.astype(jnp.bfloat16)
    value_turned = turned(project(2), 1.0)
    for part in range(2):
        block_ref[(2 + part) * half : (3 + part) * half] = value_turned[:, part * half : (part + 1) * half]
    for m in range(2):
        query_turned = turned(project(m), HEAD ** (-0.5))
        low_ref[m * 2 * HEAD : (m + 1) * 2 * HEAD] = query_turned[:, 0:half]
        high_ref[m * 2 * HEAD : (m + 1) * 2 * HEAD] = query_turned[:, half : 2 * half]

    expert_rows[...] = normalize(expert_rows[...], expert_gain_ref[...])
    slot = lax.broadcasted_iota(jnp.int32, (landed.shape[0], expert_rows.shape[0]), 0)
    match = slot == slot_ref[0:1, :]
    for k in range(1, slot_ref.shape[0]):
        match = jnp.logical_or(match, slot == slot_ref[k : k + 1, :])
    select = jnp.where(match, 1.0, 0.0).astype(jnp.bfloat16)
    width = 512
    for i in range(expert_rows.shape[1] // width):
        span = slice(i * width, (i + 1) * width)
        chosen = jnp.dot(select, expert_rows[:, span], preferred_element_type=jnp.float32)
        landed[:, span] = chosen.astype(jnp.bfloat16)
    leave = pltpu.make_async_copy(landed, leaving_ref, load_sem.at[7])
    leave.start()

    own_view = kv_ref.at[chip, core]
    along_x = [send(block_ref, own_view, send_x.at[k], recv_x.at[k], across[k]) for k in range(3)]
    own_block = pltpu.make_async_copy(block_ref, own_view, block_sem)
    own_block.start()
    asked = send(high_ref, swapped, send_query, recv_query, mirror)
    own_block.wait()
    for copy in along_x:
        copy.wait_recv()

    def level(zz, start, size):
        return kv_ref.at[pl.ds(zz * NX + start, size), core]

    pairs, along_z = [], []

    def to_other(zz, start, size, k):
        view = level(zz, start, size)
        pairs.append(send(view, view, send_pair.at[k], recv_pair.at[k], other))

    last = depth // 2
    for s in range(1, last + 1):
        parts = ((0, NX), (0, NX)) if s < last else ((0, NX // 2), (NX // 2, NX // 2))
        steps = []
        for way, peer in enumerate((up, down)):
            zz = lax.rem(z + (depth - s + 1 if way == 0 else s - 1), depth)
            view = level(zz, *parts[way])
            steps.append(send(view, view, send_z.at[s - 1, way], recv_z.at[s - 1, way], peer))
        if s == 1:
            to_other(z, 0, NX, 0)
        for way in range(2):
            steps[way].wait_recv()
            zz = lax.rem(z + (depth - s if way == 0 else s), depth)
            to_other(zz, *parts[way], 2 * s - 1 + way)
        along_z += steps
        if s == 2:
            spread.along_x()
    ring.pass_on()

    slots = leaving_ref.shape[0] // count

    def rows_of(ref, owner):
        return ref.at[pl.ds(pl.multiple_of(owner * slots, slots), slots)]

    def row_copy(k):
        peer = lax.rem(place + k, count)
        return pltpu.make_async_remote_copy(
            src_ref=rows_of(leaving_ref, peer),
            dst_ref=rows_of(landed_ref, place),
            send_sem=send_rows.at[k],
            recv_sem=recv_rows.at[k],
            device_id={"ep": peer},
            device_id_type=MESH,
        )

    def start_rows(k, carry):
        row_copy(k).start()
        return carry

    def wait_rows(k, carry):
        row_copy(k).wait()
        return carry

    leave.wait()
    lax.fori_loop(1, count, start_rows, 0)
    own_rows = pltpu.make_async_copy(rows_of(leaving_ref, place), rows_of(landed_ref, place), send_rows.at[0])
    own_rows.start()
    spread.to_other()
    for copy in pairs:
        copy.wait_recv()
    asked.wait_recv()

    rows = block_ref.shape[0] // 2
    results = (out_ref, high_part)
    attention(place, count, rows, swapped, low_ref, kv_ref, lam_ref, gain_ref, results, query, maxima, totals, weighted)
    answer = send(high_part, high_back, send_back, recv_back, mirror)

    lax.fori_loop(1, count, wait_rows, 0)
    own_rows.wait()
    fetch = pltpu.make_async_copy(landed_ref, landed, recv_rows.at[0])
    fetch.start()
    for copy in along_x + along_z + pairs + [asked, answer]:
        copy.wait_send()
    answer.wait_recv()
    out_ref[rows // 2 :, :] = high_back[...]
    fetch.wait()

    def group(owner, first):
        tile = 256

        def step(i, carry):
            span = pl.ds(pl.multiple_of(i * tile, tile), tile)
            some = landed[span, :]
            gated = jnp.dot(some, gate_all[owner], preferred_element_type=jnp.float32)
            lifted = jnp.dot(some, up_all[owner], preferred_element_type=jnp.float32)
            hidden = (gated / (1.0 + jnp.exp(-gated)) * lifted).astype(jnp.bfloat16)
            part = jnp.dot(hidden, down_all[owner], preferred_element_type=jnp.float32)
            part = part.astype(jnp.bfloat16).astype(jnp.float32)
            total[span, :] = part if first else total[span, :] + part
            return carry

        lax.fori_loop(0, landed.shape[0] // tile, step, 0)

    for copy in ring.kept:
        copy.wait()
    group(ring.me, True)
    for side in range(2):
        for i in ring.items:
            ring.own[side, 1, i].wait_recv()
        group(ring.owners[side], False)
    spread.finish()
    for i in ring.items:
        for side in range(2):
            ring.onward[side, i].wait_recv()
    group(lax.rem(ring.me + 2, ring.size), False)
    routed_ref[...] = total[...].astype(routed_ref.dtype)
    ring.finish_sends()


def attend(weights, mixer, projections, expert, slots, slot_rows, mixer_gain, expert_gain, lambdas, head_gain):
    size = lax.axis_size("tp")
    count = lax.axis_size("ep")
    half = mixer.shape[0] // 2
    width = mixer.shape[1]
    value_dim = head_gain.shape[0]
    vmem = pl.BlockSpec(memory_space=pltpu.VMEM)
    hbm = pl.BlockSpec(memory_space=pltpu.HBM)
    dma = pltpu.SemaphoreType.DMA
    steps = count // (4 * NX)
    block = jax.ShapeDtypeStruct((4 * half, value_dim), jnp.bfloat16)
    high = jax.ShapeDtypeStruct((4 * HEAD, half), jnp.bfloat16)
    leaving = jax.ShapeDtypeStruct((slot_rows, width), jnp.bfloat16)
    return pl.pallas_call(
        attend_kernel,
        out_shape=[jax.ShapeDtypeStruct((size,) + w.shape, w.dtype) for w in weights[3:]]
        + [leaving] * 3
        + [jax.ShapeDtypeStruct((2 * half, 2 * value_dim), jnp.bfloat16)],
        in_specs=[hbm] * 13 + [vmem] * 3 + [pl.BlockSpec(memory_space=pltpu.SMEM), vmem],
        out_specs=[hbm] * 5 + [vmem] * 2,
        scratch_shapes=[
            pltpu.VMEM(mixer.shape, mixer.dtype),
            pltpu.VMEM((3,) + projections[0].shape, jnp.bfloat16),
            pltpu.VMEM((2 * HEAD, width), jnp.bfloat16),
            pltpu.VMEM(expert.shape, expert.dtype),
            pltpu.VMEM(high.shape, high.dtype),
            pltpu.VMEM(high.shape, high.dtype),
            pltpu.VMEM(block.shape, block.dtype),
            dma((8,)),
        ]
        + [pltpu.VMEM((size,) + w.shape, w.dtype) for w in weights[:3]]
        + [
            pltpu.VMEM(leaving.shape, leaving.dtype),
            pltpu.VMEM(leaving.shape, jnp.float32),
            pltpu.VMEM((count // 2, 2) + block.shape, block.dtype),
            pltpu.VMEM(high.shape, high.dtype),
            pltpu.VMEM((half, 2 * value_dim), jnp.bfloat16),
            pltpu.VMEM((half, 2 * value_dim), jnp.bfloat16),
            pltpu.VMEM((2, 2, 2 * HEAD, 2 * half), jnp.bfloat16),
            pltpu.VMEM((2, 2, 1, 2 * half), jnp.float32),
            pltpu.VMEM((2, 2, 1, 2 * half), jnp.float32),
            pltpu.VMEM((2, 2, value_dim, 2 * half), jnp.float32),
            dma((3,)),
            dma((3,)),
            dma((steps, 2)),
            dma((steps, 2)),
            dma((2 * steps + 1,)),
            dma((2 * steps + 1,)),
            dma,
            dma,
            dma,
            dma,
            dma((count,)),
            dma((count,)),
            dma,
        ]
        + ring_sems(3)
        + spread_sems(size - 1, 3),
        cost_estimate=pl.CostEstimate(flops=0, bytes_accessed=300_000_000, transcendentals=0),
        compiler_params=pltpu.CompilerParams(collective_id=0, has_side_effects=True, vmem_limit_bytes=60 * 1024 * 1024),
        name="attend",
    )(
        *weights,
        mixer,
        *projections,
        expert,
        slots,
        mixer_gain.reshape(1, width),
        expert_gain.reshape(1, width),
        lambdas,
        head_gain.reshape(1, value_dim),
    )


def body(
    mixer_input,
    mixer_gain,
    query_one,
    query_two,
    key_one,
    key_two,
    value_weight,
    lambdas,
    head_gain,
    output_weight,
    expert_input,
    expert_gain,
    routes,
    route_weight,
    expert_gate,
    expert_up,
    expert_down,
    shared_gate,
    shared_up,
    shared_down,
):
    ep_size = lax.axis_size("ep")
    tp_size = lax.axis_size("tp")
    ep_rank = lax.axis_index("ep")
    mixer_rows, model_width = mixer_input.shape
    half_rows = mixer_rows // 2
    token_rows = expert_input.shape[0]

    expert_count = expert_gate.shape[0] * ep_size
    top_count = routes.shape[1]
    capacity = max(2, 5 * token_rows * top_count // (4 * expert_count))
    slot_count = expert_count * capacity
    flat_routes = routes.reshape(-1)
    onehot = (flat_routes[:, None] == jnp.arange(expert_count, dtype=jnp.int32)[None, :]).astype(jnp.bfloat16)
    before = jnp.tril(jnp.ones((token_rows * top_count, token_rows * top_count), jnp.bfloat16), -1)
    counts = jnp.dot(before, onehot, preferred_element_type=jnp.float32)
    slot_place = jnp.sum(counts * onehot, axis=1).astype(jnp.int32)
    slot_ids = (flat_routes * capacity + slot_place).reshape(token_rows, top_count)
    padded = -(-capacity // 8) * 8
    leaving_ids = (flat_routes * padded + slot_place).reshape(token_rows, top_count)
    weights = (expert_gate[0], expert_up[0], expert_down[0], shared_gate, shared_up, shared_down)
    *shared_weights, _, _, routed_result, head_rows = attend(
        weights,
        mixer_input,
        (query_one, query_two, value_weight, key_one.T, key_two.T),
        expert_input,
        leaving_ids.T,
        expert_count * padded,
        mixer_gain,
        expert_gain,
        lambdas,
        head_gain,
    )
    lines = slot_count // ep_size * model_width // 128
    routed_result = routed_result.reshape(ep_size, padded, model_width)[:, :capacity].reshape(ep_size, lines, 128)

    expert_rows, head_rows, routed_result = lax.optimization_barrier((expert_input, head_rows, routed_result))
    normed_again = normalize(expert_rows, expert_gain)
    returned = lax.all_to_all(routed_result, "ep", split_axis=0, concat_axis=0, tiled=True)
    shared_result = swiglu_groups(normed_again, *shared_weights, jnp.float32, "shared")
    partial = jnp.dot(head_rows, output_weight, preferred_element_type=jnp.float32).astype(jnp.bfloat16)
    partial = partial.reshape(tp_size, mixer_rows // tp_size, model_width)
    tp_rank = lax.axis_index("tp")
    mixer_sum = lax.dynamic_index_in_dim(partial, tp_rank, 0, keepdims=False).astype(jnp.float32)
    for step in range(1, tp_size):
        leaving = lax.dynamic_index_in_dim(partial, lax.rem(tp_rank + step, tp_size), 0, keepdims=False)
        part = lax.ppermute(leaving, "tp", [(i, (i + step) % tp_size) for i in range(tp_size)])
        mixer_sum = mixer_sum + part.astype(jnp.float32)
    mixer_output = mixer_sum.astype(jnp.bfloat16)

    returned, mixer_output, shared_result = lax.optimization_barrier((returned, mixer_output, shared_result))
    returned = returned.reshape(slot_count, model_width)
    picks = slot_ids[:, :, None] == jnp.arange(slot_count, dtype=jnp.int32)[None, None, :]
    picks = picks.astype(jnp.bfloat16)
    routed_total = jnp.zeros((token_rows, model_width), jnp.float32)
    for k in range(top_count):
        picked = jnp.dot(picks[:, k], returned, preferred_element_type=jnp.float32)
        routed_total = routed_total + picked * route_weight[:, k : k + 1]
    expert_output = (routed_total + shared_result).astype(jnp.bfloat16)
    return (mixer_output, expert_output)


def solution(mesh):
    in_specs = (
        P("ep", None),
        P(),
        P(None, "tp"),
        P(None, "tp"),
        P(None, "tp"),
        P(None, "tp"),
        P(None, "tp"),
        P("tp"),
        P(),
        P("tp", None),
        P(("ep", "tp"), None),
        P(),
        P(("ep", "tp"), None),
        P(("ep", "tp"), None),
        P("ep", None, "tp"),
        P("ep", None, "tp"),
        P("ep", "tp", None),
        P(None, "tp"),
        P(None, "tp"),
        P("tp", None),
    )
    out_specs = (P(("ep", "tp"), None), P(("ep", "tp"), None))
    return jax.shard_map(body, mesh=mesh, in_specs=in_specs, out_specs=out_specs, check_vma=False)
```

```python
import jax
import jax.numpy as jnp
from jax import lax
from jax.experimental import pallas as pl
from jax.experimental.pallas import tpu as pltpu
from jax.sharding import PartitionSpec as P

HEAD = 64

EPS = 1e-06
NEG = -1e30
MESH = pl.DeviceIdType.MESH

SPAN = 2
NX = 4


def normalize(activations, scaling):
    values = activations.astype(jnp.float32)
    factor = lax.rsqrt(jnp.mean(values * values, axis=-1, keepdims=True) + EPS)
    return (values * factor * scaling).astype(jnp.bfloat16)


def attention(rank, shards, rows, high_ref, low_ref, kv_ref, lam_ref, gain_ref, results, query, maxima, totals, weighted):
    half = rows // 2
    span_keys = SPAN * rows
    zeros = jnp.zeros((HEAD, 2 * half), jnp.bfloat16)
    for which, source in enumerate((low_ref, high_ref)):
        first = jnp.concatenate([source[0:HEAD], source[HEAD : 2 * HEAD]], axis=1)
        second = jnp.concatenate([source[2 * HEAD : 3 * HEAD], source[3 * HEAD : 4 * HEAD]], axis=1)
        query[which, 0, 0:HEAD] = first
        query[which, 0, HEAD : 2 * HEAD] = zeros
        query[which, 1, 0:HEAD] = zeros
        query[which, 1, HEAD : 2 * HEAD] = second

    def block(which, chip, masked, query_start):
        keys = kv_ref[chip, :, 0:rows, :].reshape(span_keys, 2 * HEAD)
        values = [kv_ref[chip, i, rows + j * half : rows + (j + 1) * half, :] for i in range(SPAN) for j in range(2)]
        values = jnp.concatenate(values, axis=1)
        if masked:
            key_pos = chip * span_keys + lax.broadcasted_iota(jnp.int32, (span_keys, 2 * half), 0)
            lane = lax.broadcasted_iota(jnp.int32, (span_keys, 2 * half), 1)
            query_pos = query_start + jnp.where(lane >= half, lane - half, lane)
            visible = key_pos <= query_pos
        for m in range(2):
            scores = jnp.dot(keys, query[which, m], preferred_element_type=jnp.float32)
            if masked:
                scores = jnp.where(visible, scores, NEG)
            earlier = maxima[which, m]
            latest = jnp.maximum(earlier, jnp.max(scores, axis=0, keepdims=True))
            shrink = jnp.exp(earlier - latest)
            weights = jnp.exp(scores - latest)
            if masked:
                weights = jnp.where(visible, weights, 0.0)
            totals[which, m] = totals[which, m] * shrink + jnp.sum(weights, axis=0, keepdims=True)
            product = jnp.dot(values, weights.astype(jnp.bfloat16), preferred_element_type=jnp.float32)
            weighted[which, m] = weighted[which, m] * shrink + product
            maxima[which, m] = latest

    for which in (1, 0):
        maxima[which] = jnp.full(maxima.shape[1:], NEG, jnp.float32)
        totals[which] = jnp.zeros(totals.shape[1:], jnp.float32)
        weighted[which] = jnp.zeros(weighted.shape[1:], jnp.float32)
        full = rank if which == 0 else shards - 1 - rank
        steps = full // SPAN

        def step(i, carry, which=which):
            block(which, i, False, 0)
            return carry

        lax.fori_loop(0, steps, step, 0)
        block(which, steps, True, full * rows + which * half)
        mixed = [weighted[which, m] / totals[which, m] for m in range(2)]
        lane = lax.broadcasted_iota(jnp.int32, (1, 2 * half), 1)
        combined = mixed[0] - jnp.where(lane < half, lam_ref[0], lam_ref[1]) * mixed[1]
        factor = lax.rsqrt(jnp.mean(combined * combined, axis=0, keepdims=True) + EPS)
        normed = combined * factor
        for head in range(2):
            part = normed[:, head * half : (head + 1) * half]
            results[which][0:half, head * 128 : (head + 1) * 128] = (part.T * gain_ref[...]).astype(jnp.bfloat16)


def expert_kernel(rows_ref, gate_ref, up_ref, down_ref, out_ref, total):
    group = pl.program_id(0)
    rows = rows_ref[...]
    gated = jnp.dot(rows, gate_ref[0], preferred_element_type=jnp.float32)
    lifted = jnp.dot(rows, up_ref[0], preferred_element_type=jnp.float32)
    hidden = (gated / (1.0 + jnp.exp(-gated)) * lifted).astype(jnp.bfloat16)
    part = jnp.dot(hidden, down_ref[0], preferred_element_type=jnp.float32)
    part = part.astype(jnp.bfloat16).astype(jnp.float32)

    @pl.when(group == 0)
    def _():
        total[...] = part

    @pl.when(group > 0)
    def _():
        total[...] += part

    @pl.when(group == pl.num_programs(0) - 1)
    def _():
        out_ref[...] = total[...].astype(out_ref.dtype)


def swiglu_groups(rows, gate, up, down, kind, name):
    groups, width, hidden = gate.shape
    count = rows.shape[0]
    return pl.pallas_call(
        expert_kernel,
        out_shape=jax.ShapeDtypeStruct((count, width), kind),
        grid=(groups,),
        in_specs=[
            pl.BlockSpec((count, width), lambda g: (0, 0)),
            pl.BlockSpec((1, width, hidden), lambda g: (g, 0, 0)),
            pl.BlockSpec((1, width, hidden), lambda g: (g, 0, 0)),
            pl.BlockSpec((1, hidden, width), lambda g: (g, 0, 0)),
        ],
        out_specs=pl.BlockSpec((count, width), lambda g: (0, 0)),
        scratch_shapes=[pltpu.VMEM((count, width), jnp.float32)],
        cost_estimate=pl.CostEstimate(flops=groups * count * width * hidden * 6, bytes_accessed=groups * width * hidden * 6, transcendentals=groups * count * hidden),
        compiler_params=pltpu.CompilerParams(vmem_limit_bytes=60 * 1024 * 1024),
        name=name,
    )(rows, gate, up, down)


def send(source, target, send_sem, recv_sem, peer):
    copy = pltpu.make_async_remote_copy(
        src_ref=source, dst_ref=target, send_sem=send_sem, recv_sem=recv_sem, device_id=peer, device_id_type=MESH
    )
    copy.start()
    return copy


def greet(peers, count):
    barrier = pltpu.get_barrier_semaphore()
    place = lax.axis_index("ep")
    for peer in peers:
        pl.semaphore_signal(barrier, inc=1, device_id=peer, device_id_type=MESH)

    def one(k, carry):
        peer = {"ep": lax.rem(place + k, count)}
        pl.semaphore_signal(barrier, inc=1, device_id=peer, device_id_type=MESH)
        return carry

    lax.fori_loop(1, count, one, 0)
    pl.semaphore_wait(barrier, len(peers) + count - 1)


class Ring:
    def __init__(self, sources, targets, share, sems):
        self.sources, self.targets, self.share = sources, targets, share
        self.send_own, self.recv_own, self.send_on, self.recv_on, self.local = sems
        self.size, self.me = lax.axis_size("tp"), lax.axis_index("tp")
        self.at_right = lax.rem(self.me + 1, self.size)
        self.at_left = lax.rem(self.me + self.size - 1, self.size)
        self.sides = ({"tp": self.at_right}, {"tp": self.at_left})
        self.owners = (self.at_left, self.at_right)
        self.items = range(len(sources))

    def span_of(self, i):
        rows = self.sources[i].shape[0]
        return (rows, 0) if self.share is None else (rows // 2, self.share * (rows // 2))

    def piece(self, ref, i, part):
        rows, start = self.span_of(i)
        return ref.at[pl.ds(start + part * (rows // 2), rows // 2)]

    def whole(self, ref, i):
        rows, start = self.span_of(i)
        return ref.at[pl.ds(start, rows)]

    def start(self):
        self.own, self.onward, self.kept = {}, {}, []
        for order in range(2):
            for i in self.items:
                for side in range(2):
                    part = side if order == 0 else 1 - side
                    self.own[side, order, i] = send(
                        self.piece(self.sources[i], i, part),
                        self.piece(self.targets[i].at[self.me], i, part),
                        self.send_own.at[side, order, i],
                        self.recv_own.at[side, order, i],
                        self.sides[side],
                    )
        for i in self.items:
            copy = pltpu.make_async_copy(self.sources[i], self.targets[i].at[self.me], self.local.at[i])
            copy.start()
            self.kept.append(copy)

    def pass_on(self):
        for i in self.items:
            for side in range(2):
                self.own[side, 0, i].wait_recv()
                view = self.piece(self.targets[i].at[self.owners[side]], i, side)
                self.onward[side, i] = send(
                    view, view, self.send_on.at[side, i], self.recv_on.at[side, i], self.sides[side]
                )

    def finish_sends(self):
        for i in self.items:
            for side in range(2):
                self.own[side, 0, i].wait_send()
                self.own[side, 1, i].wait_send()
                self.onward[side, i].wait_send()


def ring_sems(count):
    dma = pltpu.SemaphoreType.DMA
    return [dma((2, 2, count)), dma((2, 2, count)), dma((2, count)), dma((2, count)), dma((count,))]


class Spread:
    def __init__(self, sources, targets, x, core, tp_peers, across, other, sems):
        self.sources, self.targets, self.x, self.core = sources, targets, x, core
        self.tp_peers, self.across, self.other = tp_peers, across, other
        self.send_tp, self.recv_tp, self.send_x, self.recv_x, self.send_pair, self.recv_pair, self.local = sems
        self.me, self.size = lax.axis_index("tp"), lax.axis_size("tp")
        self.items = range(len(sources))

    def piece(self, ref, i):
        rows = self.sources[i].shape[0] // (2 * NX)
        return ref.at[pl.ds((self.core * NX + self.x) * rows, rows)]

    def start(self):
        self.first, self.kept = [], []
        for i in self.items:
            for k in range(1, self.size):
                target = self.piece(self.targets[i].at[self.me], i)
                sems = self.send_tp.at[k - 1, i], self.recv_tp.at[k - 1, i]
                self.first.append(send(self.piece(self.sources[i], i), target, *sems, self.tp_peers[k - 1]))
            copy = pltpu.make_async_copy(self.sources[i], self.targets[i].at[self.me], self.local.at[i])
            copy.start()
            self.kept.append(copy)

    def along_x(self):
        self.second = []
        for copy in self.first:
            copy.wait_recv()
        for i in self.items:
            for k in range(1, self.size):
                view = self.piece(self.targets[i].at[lax.rem(self.me + k, self.size)], i)
                for j, peer in enumerate(self.across):
                    sems = self.send_x.at[j, k - 1, i], self.recv_x.at[j, k - 1, i]
                    self.second.append(send(view, view, *sems, peer))

    def to_other(self):
        self.third = []
        for copy in self.second:
            copy.wait_recv()
        for i in self.items:
            rows = self.sources[i].shape[0] // 2
            for k in range(1, self.size):
                owner = lax.rem(self.me + k, self.size)
                view = self.targets[i].at[owner, pl.ds(self.core * rows, rows)]
                sems = self.send_pair.at[k - 1, i], self.recv_pair.at[k - 1, i]
                self.third.append(send(view, view, *sems, self.other))

    def finish(self):
        for copy in self.kept:
            copy.wait()
        for copy in self.third:
            copy.wait_recv()
        for copy in self.first + self.second + self.third:
            copy.wait_send()


def spread_sems(peers, count):
    dma = pltpu.SemaphoreType.DMA
    tp, along = (peers, count), (NX - 1, peers, count)
    return [dma(tp), dma(tp), dma(along), dma(along), dma(tp), dma(tp), dma((count,))]


def attend_kernel(
    gate_ref,
    up_ref,
    down_ref,
    shared_gate_ref,
    shared_up_ref,
    shared_down_ref,
    mixer_ref,
    query_one_ref,
    query_two_ref,
    value_ref,
    key_one_ref,
    key_two_ref,
    expert_ref,
    slot_ref,
    mixer_gain_ref,
    expert_gain_ref,
    lam_ref,
    gain_ref,
    shared_gate_out,
    shared_up_out,
    shared_down_out,
    leaving_ref,
    landed_ref,
    routed_ref,
    out_ref,
    mixer_rows,
    projections,
    key_rows,
    expert_rows,
    low_ref,
    high_ref,
    block_ref,
    load_sem,
    gate_all,
    up_all,
    down_all,
    landed,
    total,
    kv_ref,
    swapped,
    high_part,
    high_back,
    query,
    maxima,
    totals,
    weighted,
    send_x,
    recv_x,
    send_z,
    recv_z,
    send_pair,
    recv_pair,
    send_query,
    recv_query,
    send_back,
    recv_back,
    send_rows,
    recv_rows,
    block_sem,
    *sems,
):
    count = lax.axis_size("ep")
    depth = count // (2 * NX)
    place = lax.axis_index("ep")
    core = lax.rem(place, 2)
    chip = lax.div(place, 2)
    x, z = lax.rem(chip, NX), lax.div(chip, NX)

    def at(zz, xx, cc):
        return {"ep": (zz * NX + xx) * 2 + cc}

    other = at(z, x, 1 - core)
    mirror = {"ep": count - 1 - place}
    across = [at(z, lax.rem(x + k, NX), core) for k in (1, 3, 2)]
    up, down = at(lax.rem(z + 1, depth), x, core), at(lax.rem(z + depth - 1, depth), x, core)
    ring = Ring((gate_ref, up_ref, down_ref), (gate_all, up_all, down_all), None, sems[:5])
    opposite = {"tp": lax.rem(ring.me + 2, ring.size)}
    sources = (shared_gate_ref, shared_up_ref, shared_down_ref)
    targets = (shared_gate_out, shared_up_out, shared_down_out)
    tp_peers = (ring.sides[1], opposite, ring.sides[0])
    spread = Spread(sources, targets, x, core, tp_peers, across, other, sems[5:])
    loads = [(mixer_ref, mixer_rows), (expert_ref, expert_rows)]
    loads += [(w, projections.at[i]) for i, w in enumerate((query_one_ref, query_two_ref, value_ref))]
    loads += [(w, key_rows.at[pl.ds(i * HEAD, HEAD)]) for i, w in enumerate((key_one_ref, key_two_ref))]
    loads = [pltpu.make_async_copy(source, target, load_sem.at[i]) for i, (source, target) in enumerate(loads)]
    for copy in loads:
        copy.start()
    greet(ring.sides + (opposite,), count)
    spread.start()
    ring.start()
    for copy in loads[:1] + loads[2:]:
        copy.wait()

    half = mixer_rows.shape[0] // 2
    mixer_rows[...] = normalize(mixer_rows[...], mixer_gain_ref[...])
    normed = mixer_rows[...]

    def project(i):
        product = jnp.dot(normed, projections[i], preferred_element_type=jnp.float32)
        return product.astype(jnp.bfloat16)

    def turned(product, scale):
        return (product.astype(jnp.float32).T * scale).astype(jnp.bfloat16)

    keys = lax.dot_general(normed, key_rows[...], (((1,), (1,)), ((), ())), preferred_element_type=jnp.float32)
    block_ref[0 : 2 * half] = keys.astype(jnp.bfloat16)
    value_turned = turned(project(2), 1.0)
    for part in range(2):
        block_ref[(2 + part) * half : (3 + part) * half] = value_turned[:, part * half : (part + 1) * half]
    for m in range(2):
        query_turned = turned(project(m), HEAD ** (-0.5))
        low_ref[m * 2 * HEAD : (m + 1) * 2 * HEAD] = query_turned[:, 0:half]
        high_ref[m * 2 * HEAD : (m + 1) * 2 * HEAD] = query_turned[:, half : 2 * half]

    own_view = kv_ref.at[chip, core]
    along_x = [send(block_ref, own_view, send_x.at[k], recv_x.at[k], across[k]) for k in range(3)]
    own_block = pltpu.make_async_copy(block_ref, own_view, block_sem)
    own_block.start()

    loads[1].wait()
    expert_rows[...] = normalize(expert_rows[...], expert_gain_ref[...])
    slot = lax.broadcasted_iota(jnp.int32, (landed.shape[0], expert_rows.shape[0]), 0)
    match = slot == slot_ref[0:1, :]
    for k in range(1, slot_ref.shape[0]):
        match = jnp.logical_or(match, slot == slot_ref[k : k + 1, :])
    select = jnp.where(match, 1.0, 0.0).astype(jnp.bfloat16)
    width = 512
    for i in range(expert_rows.shape[1] // width):
        span = slice(i * width, (i + 1) * width)
        chosen = jnp.dot(select, expert_rows[:, span], preferred_element_type=jnp.float32)
        landed[:, span] = chosen.astype(jnp.bfloat16)
    leave = pltpu.make_async_copy(landed, leaving_ref, load_sem.at[7])
    leave.start()

    asked = send(high_ref, swapped, send_query, recv_query, mirror)
    own_block.wait()
    for copy in along_x:
        copy.wait_recv()

    def level(zz, start, size):
        return kv_ref.at[pl.ds(zz * NX + start, size), core]

    pairs, along_z = [], []

    def to_other(zz, start, size, k):
        view = level(zz, start, size)
        pairs.append(send(view, view, send_pair.at[k], recv_pair.at[k], other))

    last = depth // 2
    for s in range(1, last + 1):
        parts = ((0, NX), (0, NX)) if s < last else ((0, NX // 2), (NX // 2, NX // 2))
        steps = []
        for way, peer in enumerate((up, down)):
            zz = lax.rem(z + (depth - s + 1 if way == 0 else s - 1), depth)
            view = level(zz, *parts[way])
            steps.append(send(view, view, send_z.at[s - 1, way], recv_z.at[s - 1, way], peer))
        if s == 1:
            to_other(z, 0, NX, 0)
        for way in range(2):
            steps[way].wait_recv()
            zz = lax.rem(z + (depth - s if way == 0 else s), depth)
            to_other(zz, *parts[way], 2 * s - 1 + way)
        along_z += steps
        if s == 2:
            spread.along_x()
    ring.pass_on()

    slots = leaving_ref.shape[0] // count

    def rows_of(ref, owner):
        return ref.at[pl.ds(pl.multiple_of(owner * slots, slots), slots)]

    def row_copy(k):
        peer = lax.rem(place + k, count)
        return pltpu.make_async_remote_copy(
            src_ref=rows_of(leaving_ref, peer),
            dst_ref=rows_of(landed_ref, place),
            send_sem=send_rows.at[k],
            recv_sem=recv_rows.at[k],
            device_id={"ep": peer},
            device_id_type=MESH,
        )

    def start_rows(k, carry):
        row_copy(jnp.where(lax.rem(k, 2) == 1, lax.div(k + 1, 2), count - lax.div(k, 2))).start()
        return carry

    def wait_rows(k, carry):
        row_copy(k).wait()
        return carry

    leave.wait()
    lax.fori_loop(1, count, start_rows, 0)
    own_rows = pltpu.make_async_copy(rows_of(leaving_ref, place), rows_of(landed_ref, place), send_rows.at[0])
    own_rows.start()
    spread.to_other()
    for copy in pairs:
        copy.wait_recv()
    asked.wait_recv()

    rows = block_ref.shape[0] // 2
    results = (out_ref, high_part)
    attention(place, count, rows, swapped, low_ref, kv_ref, lam_ref, gain_ref, results, query, maxima, totals, weighted)
    answer = send(high_part, high_back, send_back, recv_back, mirror)

    lax.fori_loop(1, count, wait_rows, 0)
    own_rows.wait()
    fetch = pltpu.make_async_copy(landed_ref, landed, recv_rows.at[0])
    fetch.start()
    for copy in along_x + along_z + pairs + [asked, answer]:
        copy.wait_send()
    answer.wait_recv()
    out_ref[rows // 2 :, :] = high_back[...]
    fetch.wait()

    def group(owner, first):
        tile = 256

        def step(i, carry):
            span = pl.ds(pl.multiple_of(i * tile, tile), tile)
            some = landed[span, :]
            gated = jnp.dot(some, gate_all[owner], preferred_element_type=jnp.float32)
            lifted = jnp.dot(some, up_all[owner], preferred_element_type=jnp.float32)
            hidden = (gated / (1.0 + jnp.exp(-gated)) * lifted).astype(jnp.bfloat16)
            part = jnp.dot(hidden, down_all[owner], preferred_element_type=jnp.float32)
            part = part.astype(jnp.bfloat16).astype(jnp.float32)
            total[span, :] = part if first else total[span, :] + part
            return carry

        lax.fori_loop(0, landed.shape[0] // tile, step, 0)

    for copy in ring.kept:
        copy.wait()
    group(ring.me, True)
    for side in range(2):
        for i in ring.items:
            ring.own[side, 1, i].wait_recv()
        group(ring.owners[side], False)
    spread.finish()
    for i in ring.items:
        for side in range(2):
            ring.onward[side, i].wait_recv()
    group(lax.rem(ring.me + 2, ring.size), False)
    routed_ref[...] = total[...].astype(routed_ref.dtype)
    ring.finish_sends()


def attend(weights, mixer, projections, expert, slots, slot_rows, mixer_gain, expert_gain, lambdas, head_gain):
    size = lax.axis_size("tp")
    count = lax.axis_size("ep")
    half = mixer.shape[0] // 2
    width = mixer.shape[1]
    value_dim = head_gain.shape[0]
    vmem = pl.BlockSpec(memory_space=pltpu.VMEM)
    hbm = pl.BlockSpec(memory_space=pltpu.HBM)
    dma = pltpu.SemaphoreType.DMA
    steps = count // (4 * NX)
    block = jax.ShapeDtypeStruct((4 * half, value_dim), jnp.bfloat16)
    high = jax.ShapeDtypeStruct((4 * HEAD, half), jnp.bfloat16)
    leaving = jax.ShapeDtypeStruct((slot_rows, width), jnp.bfloat16)
    return pl.pallas_call(
        attend_kernel,
        out_shape=[jax.ShapeDtypeStruct((size,) + w.shape, w.dtype) for w in weights[3:]]
        + [leaving] * 3
        + [jax.ShapeDtypeStruct((2 * half, 2 * value_dim), jnp.bfloat16)],
        in_specs=[hbm] * 13 + [vmem] * 3 + [pl.BlockSpec(memory_space=pltpu.SMEM), vmem],
        out_specs=[hbm] * 5 + [vmem] * 2,
        scratch_shapes=[
            pltpu.VMEM(mixer.shape, mixer.dtype),
            pltpu.VMEM((3,) + projections[0].shape, jnp.bfloat16),
            pltpu.VMEM((2 * HEAD, width), jnp.bfloat16),
            pltpu.VMEM(expert.shape, expert.dtype),
            pltpu.VMEM(high.shape, high.dtype),
            pltpu.VMEM(high.shape, high.dtype),
            pltpu.VMEM(block.shape, block.dtype),
            dma((8,)),
        ]
        + [pltpu.VMEM((size,) + w.shape, w.dtype) for w in weights[:3]]
        + [
            pltpu.VMEM(leaving.shape, leaving.dtype),
            pltpu.VMEM(leaving.shape, jnp.float32),
            pltpu.VMEM((count // 2, 2) + block.shape, block.dtype),
            pltpu.VMEM(high.shape, high.dtype),
            pltpu.VMEM((half, 2 * value_dim), jnp.bfloat16),
            pltpu.VMEM((half, 2 * value_dim), jnp.bfloat16),
            pltpu.VMEM((2, 2, 2 * HEAD, 2 * half), jnp.bfloat16),
            pltpu.VMEM((2, 2, 1, 2 * half), jnp.float32),
            pltpu.VMEM((2, 2, 1, 2 * half), jnp.float32),
            pltpu.VMEM((2, 2, value_dim, 2 * half), jnp.float32),
            dma((3,)),
            dma((3,)),
            dma((steps, 2)),
            dma((steps, 2)),
            dma((2 * steps + 1,)),
            dma((2 * steps + 1,)),
            dma,
            dma,
            dma,
            dma,
            dma((count,)),
            dma((count,)),
            dma,
        ]
        + ring_sems(3)
        + spread_sems(size - 1, 3),
        cost_estimate=pl.CostEstimate(flops=0, bytes_accessed=300_000_000, transcendentals=0),
        compiler_params=pltpu.CompilerParams(collective_id=0, has_side_effects=True, vmem_limit_bytes=60 * 1024 * 1024),
        name="attend",
    )(
        *weights,
        mixer,
        *projections,
        expert,
        slots,
        mixer_gain.reshape(1, width),
        expert_gain.reshape(1, width),
        lambdas,
        head_gain.reshape(1, value_dim),
    )


def body(
    mixer_input,
    mixer_gain,
    query_one,
    query_two,
    key_one,
    key_two,
    value_weight,
    lambdas,
    head_gain,
    output_weight,
    expert_input,
    expert_gain,
    routes,
    route_weight,
    expert_gate,
    expert_up,
    expert_down,
    shared_gate,
    shared_up,
    shared_down,
):
    ep_size = lax.axis_size("ep")
    tp_size = lax.axis_size("tp")
    ep_rank = lax.axis_index("ep")
    mixer_rows, model_width = mixer_input.shape
    half_rows = mixer_rows // 2
    token_rows = expert_input.shape[0]

    expert_count = expert_gate.shape[0] * ep_size
    top_count = routes.shape[1]
    capacity = max(2, 5 * token_rows * top_count // (4 * expert_count))
    slot_count = expert_count * capacity
    flat_routes = routes.reshape(-1)
    onehot = (flat_routes[:, None] == jnp.arange(expert_count, dtype=jnp.int32)[None, :]).astype(jnp.bfloat16)
    before = jnp.tril(jnp.ones((token_rows * top_count, token_rows * top_count), jnp.bfloat16), -1)
    counts = jnp.dot(before, onehot, preferred_element_type=jnp.float32)
    slot_place = jnp.sum(counts * onehot, axis=1).astype(jnp.int32)
    slot_ids = (flat_routes * capacity + slot_place).reshape(token_rows, top_count)
    padded = -(-capacity // 8) * 8
    leaving_ids = (flat_routes * padded + slot_place).reshape(token_rows, top_count)
    weights = (expert_gate[0], expert_up[0], expert_down[0], shared_gate, shared_up, shared_down)
    *shared_weights, _, _, routed_result, head_rows = attend(
        weights,
        mixer_input,
        (query_one, query_two, value_weight, key_one.T, key_two.T),
        expert_input,
        leaving_ids.T,
        expert_count * padded,
        mixer_gain,
        expert_gain,
        lambdas,
        head_gain,
    )
    lines = slot_count // ep_size * model_width // 128
    routed_result = routed_result.reshape(ep_size, padded, model_width)[:, :capacity].reshape(ep_size, lines, 128)

    expert_rows, head_rows, routed_result = lax.optimization_barrier((expert_input, head_rows, routed_result))
    normed_again = normalize(expert_rows, expert_gain)
    returned = lax.all_to_all(routed_result, "ep", split_axis=0, concat_axis=0, tiled=True)
    shared_result = swiglu_groups(normed_again, *shared_weights, jnp.float32, "shared")
    partial = jnp.dot(head_rows, output_weight, preferred_element_type=jnp.float32).astype(jnp.bfloat16)
    partial = partial.reshape(tp_size, mixer_rows // tp_size, model_width)
    tp_rank = lax.axis_index("tp")
    mixer_sum = lax.dynamic_index_in_dim(partial, tp_rank, 0, keepdims=False).astype(jnp.float32)
    for step in range(1, tp_size):
        leaving = lax.dynamic_index_in_dim(partial, lax.rem(tp_rank + step, tp_size), 0, keepdims=False)
        part = lax.ppermute(leaving, "tp", [(i, (i + step) % tp_size) for i in range(tp_size)])
        mixer_sum = mixer_sum + part.astype(jnp.float32)
    mixer_output = mixer_sum.astype(jnp.bfloat16)

    returned, mixer_output, shared_result = lax.optimization_barrier((returned, mixer_output, shared_result))
    returned = returned.reshape(slot_count, model_width)
    picks = slot_ids[:, :, None] == jnp.arange(slot_count, dtype=jnp.int32)[None, None, :]
    picks = picks.astype(jnp.bfloat16)
    routed_total = jnp.zeros((token_rows, model_width), jnp.float32)
    for k in range(top_count):
        picked = jnp.dot(picks[:, k], returned, preferred_element_type=jnp.float32)
        routed_total = routed_total + picked * route_weight[:, k : k + 1]
    expert_output = (routed_total + shared_result).astype(jnp.bfloat16)
    return (mixer_output, expert_output)


def solution(mesh):
    in_specs = (
        P("ep", None),
        P(),
        P(None, "tp"),
        P(None, "tp"),
        P(None, "tp"),
        P(None, "tp"),
        P(None, "tp"),
        P("tp"),
        P(),
        P("tp", None),
        P(("ep", "tp"), None),
        P(),
        P(("ep", "tp"), None),
        P(("ep", "tp"), None),
        P("ep", None, "tp"),
        P("ep", None, "tp"),
        P("ep", "tp", None),
        P(None, "tp"),
        P(None, "tp"),
        P("tp", None),
    )
    out_specs = (P(("ep", "tp"), None), P(("ep", "tp"), None))
    return jax.shard_map(body, mesh=mesh, in_specs=in_specs, out_specs=out_specs, check_vma=False)
```
